128 devices in a mesh: fs: 16 (over z, x), tp: 8 (over y, core).
Axes of the slice: x: 4, y: 4, z: 4, core: 2. Of those that a mesh axis runs over, the one named last changes fastest.
Arguments:
- tokens: bfloat16 [16384, 2048], P('fs', 'tp'), may hold values from -17 to 17
- first_gain: float32 [2048], replicated, may hold values from 0.1 to 1.9
- first_gate: bfloat16 [2048, 5120], P('fs', 'tp'), may hold values from -0.125 to 0.125
- first_up: bfloat16 [2048, 5120], P('fs', 'tp'), may hold values from -0.125 to 0.125
- first_down: bfloat16 [2048, 5120], P('fs', 'tp'), may hold values from -0.078125 to 0.078125
- mix_gain: float32 [2048], replicated, may hold values from 0.1 to 1.9
- mix_input: bfloat16 [2048, 1024], P('fs', 'tp'), may hold values from -0.125 to 0.125
- mix_branch: bfloat16 [2048, 1024], P('fs', 'tp'), may hold values from -0.125 to 0.125
- conv_weight: bfloat16 [4, 1024], P(None, 'tp'), may hold values from -3 to 3
- rate_weight: bfloat16 [16, 64, 64], P('tp'), may hold values from -0.75 to 0.75
- input_weight: bfloat16 [16, 64, 64], P('tp'), may hold values from -0.75 to 0.75
- decay_param: float32 [1024], P('tp'), may hold values from 3 to 11
- decay_shift: float32 [16384, 16], P('fs', 'tp'), may hold values from -1.5 to 0
- mix_output: bfloat16 [2048, 1024], P('fs', 'tp'), may hold values from -0.1875 to 0.1875
- second_gain: float32 [2048], replicated, may hold values from 0.1 to 1.9
- second_gate: bfloat16 [2048, 5120], P('fs', 'tp'), may hold values from -0.125 to 0.125
- second_up: bfloat16 [2048, 5120], P('fs', 'tp'), may hold values from -0.125 to 0.125
- second_down: bfloat16 [2048, 5120], P('fs', 'tp'), may hold values from -0.078125 to 0.078125
- final_gain: float32 [2048], P('tp'), may hold values from 0.1 to 1.9
Outputs:
- output: bfloat16 [16384, 2048], P('fs', 'tp')
The draws below stay inside these ranges and needn't reach their ends.
All inputs are finite; a program needn't handle non-finite values.
Results may differ from the reference program's by a relative error of at most 0.019.
Values may be sent and summed in bfloat16 or wider, within the bound.
No kernel may reach another device: no remote copies, remote signals or barrier semaphores. Data moves between devices by JAX's collectives and lax.ppermute only.
A program may use at most 128 MiB of HBM per device.

```python
import math
import jax
import jax.numpy as jnp
from jax import lax

D = 2048
FF = 5120
LANE_GROUPINGS = 16
HEAD_DIM = 64
CONV = 4
SEQ = 1024
LRU = 1024
SYMBOL_TOTAL = 16384
N_TP = 8


def draw_tokens(key, part):
    key_base, key_rows = jax.random.split(key, 2)
    starting_number = jnp.clip(jax.random.normal(key_base, (SYMBOL_TOTAL, D), jnp.float32), -4.0, 4.0)
    rows = jnp.exp(jax.random.uniform(key_rows, (SYMBOL_TOTAL, 1), jnp.float32, 0.0, math.log(4.0)))
    columns = jnp.exp(math.log(3.0) * jnp.arange(D, dtype=jnp.float32) / D)
    return (0.25 * starting_number * rows * columns[None, :]).astype(jnp.bfloat16)


def draw_decay_param(key, part):
    key_pick, key_rate = jax.random.split(key, 2)
    share = 0.5
    picked = jax.random.uniform(key_pick, (LRU,), jnp.float32) < share
    unit = jax.random.uniform(key_rate, (LRU,), jnp.float32)
    slow = jnp.exp(math.log(0.5) + unit * math.log(4.0)) / (4.0 * SEQ)
    fast = jnp.exp(math.log(1.0 / 120.0) + unit * math.log(5.0))
    speed = jnp.where(picked, slow, fast)
    return -speed - jnp.log(-jnp.expm1(-speed))


def draw_decay_shift(key, part):
    key_base, key_spot, key_depth = jax.random.split(key, 3)
    count = SYMBOL_TOTAL // SEQ
    starting_number = -jnp.exp(jax.random.uniform(key_base, (count, 1, LANE_GROUPINGS), jnp.float32, math.log(0.1), math.log(0.5))) / SEQ
    location_marks = jax.random.randint(key_spot, (count, 2, 1), 0, SEQ)
    layer_ordinal = jnp.log(jax.random.uniform(key_depth, (count, 2, 1), jnp.float32, 0.5, 0.8))
    position_holders = jnp.arange(SEQ, dtype=jnp.int32)[None, None, :]
    repeated_spans = jnp.sum(jnp.where(location_marks == position_holders, layer_ordinal, 0.0), axis=1)
    return (starting_number + repeated_spans[:, :, None]).reshape(SYMBOL_TOTAL, LANE_GROUPINGS)


def steps_of(own_key, extent, pieces, low, largest):
    loudness, own = 1.0, jax.random.fold_in(own_key, 6)
    for axis_at, parts in pieces:
        steps = jnp.exp(jax.random.uniform(jax.random.fold_in(own, axis_at), (parts,), jnp.float32, low / len(pieces), largest / len(pieces)))
        loudness = loudness * jnp.repeat(steps, extent[axis_at] // parts).reshape([-1 if axis == axis_at else 1 for axis in range(len(extent))])
    return loudness


def noise(own_key, shape, spread, bound, cuts=(), kind=jnp.bfloat16):
    entries = jax.random.normal(own_key, shape, jnp.float32) * spread
    if len(cuts) > 0:
        entries = steps_of(own_key, shape, cuts, -0.22, 0.18) * entries
    return jnp.clip(entries, min=-bound, max=bound).astype(kind)


def setup_inputs(seed: int = 0) -> dict:
    streams_of = jax.random.split(jax.random.key(seed), 20)
    tokens = draw_tokens(jax.random.fold_in(streams_of[19], 71), 0)
    first_gain = jnp.clip(1.0 + 0.18 * jax.random.normal(streams_of[1], (D,), jnp.float32), 0.1, 1.9)
    first_gate = noise(streams_of[2], (D, FF), D ** -0.5, 0.125, ((0, 16), (1, 8)))
    first_up = noise(streams_of[3], (D, FF), D ** -0.5, 0.125, ((0, 16), (1, 8)))
    first_down = noise(streams_of[4], (D, FF), FF ** -0.5, 0.078125, ((0, 16), (1, 8)))
    mix_gain = jnp.clip(1.0 + 0.18 * jax.random.normal(streams_of[5], (D,), jnp.float32), 0.1, 1.9)
    mix_input = noise(streams_of[6], (D, LRU), D ** -0.5, 0.125, ((0, 16), (1, 8)))
    mix_branch = noise(streams_of[7], (D, LRU), D ** -0.5, 0.125, ((0, 16), (1, 8)))
    conv_weight = noise(streams_of[8], (CONV, LRU), CONV ** -0.5, 3.0, ((1, 8),))
    rate_weight = noise(streams_of[9], (LANE_GROUPINGS, HEAD_DIM, HEAD_DIM), HEAD_DIM ** -0.5, 0.75, ((0, 8),))
    input_weight = noise(streams_of[10], (LANE_GROUPINGS, HEAD_DIM, HEAD_DIM), HEAD_DIM ** -0.5, 0.75, ((0, 8),))
    decay_param = draw_decay_param(jax.random.fold_in(streams_of[19], 71), 0)
    decay_shift = draw_decay_shift(jax.random.fold_in(streams_of[19], 71), 0)
    mix_output = noise(streams_of[13], (D, LRU), LRU ** -0.5, 0.1875, ((0, 16), (1, 8)))
    second_gain = jnp.clip(1.0 + 0.18 * jax.random.normal(streams_of[14], (D,), jnp.float32), 0.1, 1.9)
    second_gate = noise(streams_of[15], (D, FF), D ** -0.5, 0.125, ((0, 16), (1, 8)))
    second_up = noise(streams_of[16], (D, FF), D ** -0.5, 0.125, ((0, 16), (1, 8)))
    second_down = noise(streams_of[17], (D, FF), FF ** -0.5, 0.078125, ((0, 16), (1, 8)))
    final_gain = jnp.clip(1.0 + 0.18 * jax.random.normal(streams_of[18], (D,), jnp.float32), 0.1, 1.9)
    return dict(tokens=tokens, first_gain=first_gain, first_gate=first_gate, first_up=first_up, first_down=first_down, mix_gain=mix_gain, mix_input=mix_input, mix_branch=mix_branch, conv_weight=conv_weight, rate_weight=rate_weight, input_weight=input_weight, decay_param=decay_param, decay_shift=decay_shift, mix_output=mix_output, second_gain=second_gain, second_gate=second_gate, second_up=second_up, second_down=second_down, final_gain=final_gain)


norm_eps = 1e-06
rate_scale = 8.0

def rms_rows(rows, gain):
    values = rows.astype(jnp.float32)
    scale = lax.rsqrt(lax.optimization_barrier(jnp.mean(values * values, axis=-1, keepdims=True)) + norm_eps)
    return (values * scale * gain).astype(jnp.bfloat16)

def group_terms(left, weight):
    width = left.shape[1] // N_TP
    total = jnp.zeros((left.shape[0], weight.shape[0]), jnp.float32)
    for group in range(N_TP):
        piece = left[:, group * width:(group + 1) * width]
        weight_piece = weight[:, group * width:(group + 1) * width]
        term = lax.dot_general(piece, weight_piece, (((1,), (1,)), ((), ())), preferred_element_type=jnp.float32)
        total = total + lax.optimization_barrier(term.astype(jnp.bfloat16)).astype(jnp.float32)
    return total

def half_step(stream, gain, weight_gate, weight_up, weight_down):
    normed = rms_rows(stream, gain)
    gate_value = jnp.dot(normed, weight_gate, preferred_element_type=jnp.float32)
    up_value = jnp.dot(normed, weight_up, preferred_element_type=jnp.float32)
    hidden = (jax.nn.silu(gate_value) * up_value).astype(jnp.bfloat16)
    return (stream.astype(jnp.float32) + 0.5 * group_terms(hidden, weight_down)).astype(jnp.bfloat16)

def combine_steps(earlier, later):
    return (earlier[0] * later[0], later[0] * earlier[1] + later[1])

def lane_mixer(stream, gain, mix_input, mix_branch, conv_weight, rate_weight, input_weight, decay_param, decay_shift, mix_output):
    normed = rms_rows(stream, gain)
    lane_input = jnp.dot(normed, mix_input, preferred_element_type=jnp.float32).astype(jnp.bfloat16)
    branch_value = jnp.dot(normed, mix_branch, preferred_element_type=jnp.float32)
    width = lane_input.shape[1]
    lanes = lane_input.reshape(-1, SEQ, width).astype(jnp.float32)
    count = lanes.shape[0]
    padded = jnp.pad(lanes, ((0, 0), (CONV - 1, 0), (0, 0)))
    conv_sum = jnp.zeros_like(lanes)
    for offset in range(CONV):
        conv_sum = conv_sum + padded[:, offset:offset + SEQ] * conv_weight[offset].astype(jnp.float32)
    conv_out = conv_sum.astype(jnp.bfloat16)
    blocks = conv_out.reshape(count, SEQ, -1, HEAD_DIM).astype(jnp.float32)
    rate = jax.nn.sigmoid(jnp.einsum('nshd,hde->nshe', blocks, rate_weight.astype(jnp.float32))).reshape(lanes.shape)
    admit = jax.nn.sigmoid(jnp.einsum('nshd,hde->nshe', blocks, input_weight.astype(jnp.float32))).reshape(lanes.shape)
    shift = jnp.repeat(decay_shift.reshape(count, SEQ, -1), HEAD_DIM, axis=-1)
    log_decay = rate_scale * rate * jax.nn.log_sigmoid(decay_param) + shift
    drive = jnp.sqrt(-jnp.expm1(2.0 * log_decay)) * admit * conv_out.astype(jnp.float32)
    _, state = lax.associative_scan(combine_steps, (jnp.exp(log_decay), drive), axis=1)
    mixed_lane = (state.reshape(-1, width) * jax.nn.gelu(branch_value)).astype(jnp.bfloat16)
    return (stream.astype(jnp.float32) + group_terms(mixed_lane, mix_output)).astype(jnp.bfloat16)

def reference(tokens, first_gain, first_gate, first_up, first_down, mix_gain, mix_input, mix_branch, conv_weight, rate_weight, input_weight, decay_param, decay_shift, mix_output, second_gain, second_gate, second_up, second_down, final_gain):
    stream = half_step(tokens, first_gain, first_gate, first_up, first_down)
    stream = lane_mixer(stream, mix_gain, mix_input, mix_branch, conv_weight, rate_weight, input_weight, decay_param, decay_shift, mix_output)
    stream = half_step(stream, second_gain, second_gate, second_up, second_down)
    values = stream.astype(jnp.float32)
    scale = lax.rsqrt(lax.optimization_barrier(jnp.mean(values * values, axis=-1, keepdims=True)) + norm_eps)
    return (values * scale * final_gain).astype(jnp.bfloat16)
```

```python
import functools

import jax
import jax.numpy as jnp
from jax import lax
from jax.experimental import pallas as pl
from jax.experimental.pallas import tpu as pltpu
from jax.sharding import Mesh
from jax.sharding import PartitionSpec as P

D = 2048
BLK = 256
HEAD_DIM = 64
CONV = 4
TP = ("tp_0", "tp_1")
norm_eps = 1e-06
rate_scale = 8.0
bf16 = jnp.bfloat16
f32 = jnp.float32


OFFSETS = ((0, 0), (0, 1), (1, 0), (1, 1), (-1, 0), (-1, 1), (2, 0), (2, 1))


def ring(value, step):
    return lax.ppermute(value, "tp_0", [(i, (i + step) % 4) for i in range(4)])


def swap(value):
    return lax.ppermute(value, "tp_1", [(0, 1), (1, 0)])


def gather_row_blocks(block):
    half = block.shape[0] // 2
    left = ring(block, 1)
    right = ring(block, -1)
    other = swap(block)
    far_top = ring(left[:half], 1)
    far_low = ring(right[half:], -1)
    return (
        (block, other, right, swap(right), left, swap(left)),
        (far_top, far_low, swap(far_top), swap(far_low)),
    )


def scatter_row_blocks(parts):
    half = parts[0].shape[0] // 2
    sent = [swap(parts[k]) for k in (7, 3, 5, 1)]
    far, right, left, own = [
        parts[k].astype(f32) + s.astype(f32) for k, s in zip((6, 2, 4, 0), sent)
    ]
    far = far.astype(bf16)
    got_right = ring(far[:half], 1)
    got_left = ring(far[half:], -1)
    right = jnp.concatenate([right[:half] + got_right.astype(f32), right[half:]], 0).astype(bf16)
    left = jnp.concatenate([left[:half], left[half:] + got_left.astype(f32)], 0).astype(bf16)
    return own + ring(right, 1).astype(f32) + ring(left, -1).astype(f32)


def owners():
    y, c = lax.axis_index("tp_0"), lax.axis_index("tp_1")
    return jnp.stack([((y + dy) % 4) * 2 + (c + dc) % 2 for dy, dc in OFFSETS]).astype(jnp.int32)


def norm_into(x_refs, far_refs, at_ref, gain_ref, normed_ref, rows):
    half = rows // 2
    step = min(256, half)
    for lo in range(0, rows, step):
        span = slice(lo, lo + step)
        top = lo < half
        fspan = slice(lo, lo + step) if top else slice(lo - half, lo - half + step)
        far_a = far_refs[0 if top else 1]
        far_b = far_refs[2 if top else 3]
        blocks = [r[span, :].astype(f32) for r in x_refs]
        blocks += [far_a[fspan, :].astype(f32), far_b[fspan, :].astype(f32)]
        square = blocks[0] * blocks[0]
        for b in blocks[1:]:
            square = square + b * b
        scale = lax.rsqrt(jnp.sum(square, axis=1, keepdims=True) / D + norm_eps)
        for k, b in enumerate(blocks):
            at = at_ref[k]
            lane = pl.multiple_of(at * BLK, BLK)
            normed_ref[span, pl.ds(lane, BLK)] = (b * scale * gain_ref[at]).astype(bf16)


def dot_t(left, right):
    return lax.dot_general(left, right, (((1,), (1,)), ((), ())), preferred_element_type=f32)


def half_step_kernel(at_ref, *refs, rows):
    x_refs, far_refs = refs[0:6], refs[6:10]
    gain_ref, weight_ref = refs[10:12]
    outs = refs[12:20]
    normed_ref, hidden_ref = refs[20:22]
    width = weight_ref.shape[1] // 3
    norm_into(x_refs, far_refs, at_ref, gain_ref, normed_ref, rows)
    step = min(512, rows)
    for lo in range(0, rows, step):
        normed = normed_ref[lo : lo + step, :]
        both = jnp.dot(normed, weight_ref[:, : 2 * width], preferred_element_type=f32)
        gate, up = both[:, :width], both[:, width:]
        hidden_ref[lo : lo + step, :] = (gate * jax.nn.sigmoid(gate) * up).astype(bf16)
    for k in (7, 3, 5, 1, 6, 2, 4, 0):
        at = pl.multiple_of(at_ref[k] * BLK, BLK)
        down = weight_ref[pl.ds(at, BLK), 2 * width :]
        outs[k][...] = dot_t(hidden_ref[...], down).astype(bf16)


def one_minus_exp(value):
    small = jnp.zeros_like(value)
    for n in (8, 7, 6, 5, 4, 3, 2):
        small = value * (1.0 / n) * (1.0 + small)
    small = value * (1.0 + small)
    return jnp.where(value > -0.5, -small, 1.0 - jnp.exp(value))


def shifted(value, by, fill):
    rows = value.shape[0]
    if by % 8 == 0:
        head = jnp.full((by, value.shape[1]), fill, value.dtype)
        return jnp.concatenate([head, value[: rows - by]], axis=0)
    rolled = pltpu.roll(value, by, 0)
    at = lax.broadcasted_iota(jnp.int32, value.shape, 0)
    return jnp.where(at < by, fill, rolled)


def mixer_kernel(at_ref, *refs, rows):
    x_refs, far_refs = refs[0:6], refs[6:10]
    gain_ref, weight_ref, conv_ref, rate_ref, input_ref, slope_ref, shift_ref = refs[10:17]
    outs = refs[17:25]
    normed_ref, mixed_ref = refs[25:27]
    width = weight_ref.shape[1] // 3
    norm_into(x_refs, far_refs, at_ref, gain_ref, normed_ref, rows)
    both = jnp.dot(normed_ref[...], weight_ref[:, : 2 * width], preferred_element_type=f32)
    lane = both[:, :width].astype(bf16).astype(f32)
    branch = both[:, width:]
    conv = lane * conv_ref[CONV - 1].astype(f32)
    for back in range(1, CONV):
        conv = conv + shifted(lane, back, 0.0) * conv_ref[CONV - 1 - back].astype(f32)
    conv = conv.astype(bf16)
    rate = jax.nn.sigmoid(jnp.dot(conv, rate_ref[...], preferred_element_type=f32))
    admit = jax.nn.sigmoid(jnp.dot(conv, input_ref[...], preferred_element_type=f32))
    at = lax.broadcasted_iota(jnp.int32, (rows, width), 1)
    shift = jnp.where(at < HEAD_DIM, shift_ref[:, 0:1], shift_ref[:, 1:2])
    log_decay = rate_scale * rate * slope_ref[...] + shift
    state = jnp.sqrt(one_minus_exp(2.0 * log_decay)) * admit * conv.astype(f32)
    decay = jnp.exp(log_decay)
    by = 1
    while by < rows:
        state = state + decay * shifted(state, by, 0.0)
        if by * 2 < rows:
            decay = decay * shifted(decay, by, 1.0)
        by *= 2
    gelu = jax.nn.gelu(branch)
    mixed_ref[...] = (state * gelu).astype(bf16)
    for k in (7, 3, 5, 1, 6, 2, 4, 0):
        at = pl.multiple_of(at_ref[k] * BLK, BLK)
        outs[k][...] = dot_t(mixed_ref[...], weight_ref[pl.ds(at, BLK), 2 * width :]).astype(bf16)


def call(kernel, at, operands, rows, width, name):
    vmem = pl.BlockSpec(memory_space=pltpu.VMEM)
    return pl.pallas_call(
        functools.partial(kernel, rows=rows),
        out_shape=[jax.ShapeDtypeStruct((rows, BLK), bf16)] * 8,
        in_specs=[pl.BlockSpec(memory_space=pltpu.SMEM)] + [vmem] * len(operands),
        out_specs=[vmem] * 8,
        scratch_shapes=[pltpu.VMEM((rows, D), bf16), pltpu.VMEM((rows, width), bf16)],
        compiler_params=pltpu.CompilerParams(vmem_limit_bytes=50 * 1024 * 1024),
        name=name,
    )(at, *operands)


def gathered(arrays):
    both = jnp.concatenate(arrays, axis=1)
    return lax.all_gather(both, "fs", axis=0, tiled=True)


def block_map(weight):
    zero = jnp.zeros((HEAD_DIM, HEAD_DIM), weight.dtype)
    return jnp.block([[weight[0], zero], [zero, weight[1]]])


def shards(
    tokens,
    first_gain,
    first_gate,
    first_up,
    first_down,
    mix_gain,
    mix_input,
    mix_branch,
    conv_weight,
    rate_weight,
    input_weight,
    decay_param,
    decay_shift,
    mix_output,
    second_gain,
    second_gate,
    second_up,
    second_down,
    final_gain,
):
    rows = tokens.shape[0]
    at = owners()
    first = gathered((first_gate, first_up, first_down))
    mix = gathered((mix_input, mix_branch, mix_output))
    second = gathered((second_gate, second_up, second_down))
    gains = [g.reshape(8, 1, BLK) for g in (first_gain, mix_gain, second_gain)]
    slope = jax.nn.log_sigmoid(decay_param).reshape(1, -1)
    rate_map, input_map = block_map(rate_weight), block_map(input_weight)

    def half(stream, gain, weight):
        near, far = gather_row_blocks(stream)
        parts = call(
            half_step_kernel, at, (*near, *far, gain, weight), rows, weight.shape[1] // 3, "half_step"
        )
        total = scatter_row_blocks(parts)
        return stream.astype(f32) + 0.5 * total

    stream = half(tokens, gains[0], first).astype(bf16)
    near, far = gather_row_blocks(stream)
    parts = call(
        mixer_kernel,
        at,
        (*near, *far, gains[1], mix, conv_weight, rate_map, input_map, slope, decay_shift),
        rows,
        mix.shape[1] // 3,
        "mixer",
    )
    stream = (stream.astype(f32) + scatter_row_blocks(parts)).astype(bf16)
    values = half(stream, gains[2], second).astype(bf16).astype(f32)
    mine = jnp.sum(values * values, axis=1)
    pair = mine + swap(mine)
    square = pair + ring(pair, 1) + ring(pair, -1) + ring(pair, 2)
    scale = lax.rsqrt(square / D + norm_eps)
    return (values * scale[:, None] * final_gain).astype(bf16)


def solution(mesh):
    finer = Mesh(mesh.devices.reshape(mesh.shape["fs"], 4, 2), ("fs", "tp_0", "tp_1"))
    placed = (
        P("fs", TP),
        P(),
        P("fs", TP),
        P("fs", TP),
        P("fs", TP),
        P(),
        P("fs", TP),
        P("fs", TP),
        P(None, TP),
        P(TP, None, None),
        P(TP, None, None),
        P(TP),
        P("fs", TP),
        P("fs", TP),
        P(),
        P("fs", TP),
        P("fs", TP),
        P("fs", TP),
        P(TP),
    )
    return jax.shard_map(
        shards, mesh=finer, in_specs=placed, out_specs=P("fs", TP), check_vma=False
    )
```

```python
import functools

import jax
import jax.numpy as jnp
from jax import lax
from jax.experimental import pallas as pl
from jax.experimental.pallas import tpu as pltpu
from jax.sharding import Mesh
from jax.sharding import PartitionSpec as P


D = 2048
BLK = 256
HEAD_DIM = 64
CONV = 4
TP = ("tp_0", "tp_1")
norm_eps = 1e-06
rate_scale = 8.0
bf16 = jnp.bfloat16
f32 = jnp.float32


OFFSETS = ((0, 0), (0, 1), (1, 0), (1, 1), (-1, 0), (-1, 1), (2, 0), (2, 1))


def ring(value, step):
    return lax.ppermute(value, "tp_0", [(i, (i + step) % 4) for i in range(4)])


def swap(value):
    return lax.ppermute(value, "tp_1", [(0, 1), (1, 0)])


def gather_row_blocks(block):
    half = block.shape[0] // 2
    top, low = block[:half], block[half:]
    left_top = ring(top, 1)
    right_low = ring(low, -1)
    left_low = ring(low, 1)
    right_top = ring(top, -1)
    far_top = ring(left_top, 1)
    far_low = ring(right_low, -1)
    halves = (right_top, right_low, left_top, left_low, far_top, far_low)
    other = swap(block)
    swapped = [swap(h) for h in halves]
    blocks = [block, other]
    for k in range(0, 6, 2):
        blocks += [*halves[k : k + 2], *swapped[k : k + 2]]
    return tuple(blocks)


def scatter_row_blocks(mine, others):
    half = mine.shape[1] // 2
    got = swap(others)
    own, right, left, far = [mine[k].astype(f32) + got[k].astype(f32) for k in range(4)]
    far = far.astype(bf16)
    got_right = ring(far[:half], 1)
    got_left = ring(far[half:], -1)
    right_low = ring(right[half:].astype(bf16), 1)
    left_top = ring(left[:half].astype(bf16), -1)
    right_top = ring((right[:half] + got_right.astype(f32)).astype(bf16), 1)
    left_low = ring((left[half:] + got_left.astype(f32)).astype(bf16), -1)
    top = own[:half] + right_top.astype(f32) + left_top.astype(f32)
    low = own[half:] + right_low.astype(f32) + left_low.astype(f32)
    return jnp.concatenate([top, low], axis=0)


def fs_ring(value, dz, dx):
    pairs = [
        (z * 4 + x, ((z + dz) % 4) * 4 + (x + dx) % 4) for z in range(4) for x in range(4)
    ]
    return lax.ppermute(value, "fs", pairs)


def put(whole, piece, *start):
    return lax.dynamic_update_slice(whole, piece, start)


def gather_rows_by_permute(first, second):
    z, x = lax.axis_index("fs") // 4, lax.axis_index("fs") % 4
    rows = first.shape[0]
    a_got = [(0, first)]
    b_got = [(0, second)]
    for step in (1, -1, 2):
        a_got.append((step, fs_ring(first, 0, step)))
        b_got.append((step, fs_ring(second, step, 0)))
    a_line = jnp.zeros((4, *first.shape), bf16)
    b_line = jnp.zeros((4, *second.shape), bf16)
    for step, piece in a_got:
        a_line = put(a_line, piece[None], (x - step) % 4, 0, 0)
    for step, piece in b_got:
        b_line = put(b_line, piece[None], (z - step) % 4, 0, 0)
    a_left = fs_ring(a_line, 1, 0)
    a_right = fs_ring(a_line, -1, 0)
    b_left = fs_ring(b_line, 0, 1)
    b_right = fs_ring(b_line, 0, -1)
    a_far = (fs_ring(a_left[:2], 1, 0), fs_ring(a_right[2:], -1, 0))
    b_far = (fs_ring(b_left[:2], 0, 1), fs_ring(b_right[2:], 0, -1))
    a = jnp.zeros((4, 4, *first.shape), bf16)
    b = jnp.zeros((4, 4, *second.shape), bf16)
    for step, lo, piece in (
        (0, 0, a_line),
        (-1, 0, a_left),
        (1, 0, a_right),
        (2, 0, a_far[0]),
        (2, 2, a_far[1]),
    ):
        a = put(a, piece[None], (z + step) % 4, lo, 0, 0)
    for step, lo, piece in (
        (0, 0, b_line),
        (-1, 0, b_left),
        (1, 0, b_right),
        (2, 0, b_far[0]),
        (2, 2, b_far[1]),
    ):
        b = put(b, piece[:, None], lo, (x + step) % 4, 0, 0)
    return a.reshape(16 * rows, -1), b.reshape(16 * rows, -1)


def owners():
    y, c = lax.axis_index("tp_0"), lax.axis_index("tp_1")
    return jnp.stack([((y + dy) % 4) * 2 + (c + dc) % 2 for dy, dc in OFFSETS]).astype(jnp.int32)


def norm_into(x_refs, at_ref, gain_ref, normed_ref, rows):
    half = rows // 2
    step = min(256, half)
    for side in range(2):
        refs = [*x_refs[:2]] + [x_refs[2 + 2 * k + side] for k in range(6)]

        def body(i, carry, side=side, refs=refs):
            near = pl.ds(pl.multiple_of(side * half + i * step, step), step)
            piece = pl.ds(pl.multiple_of(i * step, step), step)
            spans = [near, near] + [piece] * 6
            square = None
            for r, span in zip(refs, spans):
                v = r[span, :].astype(f32)
                square = v * v if square is None else square + v * v
            scale = lax.rsqrt(jnp.sum(square, axis=1, keepdims=True) / D + norm_eps)
            for k, (r, span) in enumerate(zip(refs, spans)):
                at = at_ref[k]
                lane = pl.ds(pl.multiple_of(at * BLK, BLK), BLK)
                normed_ref[near, lane] = (r[span, :].astype(f32) * scale * gain_ref[at]).astype(bf16)
            return carry

        lax.fori_loop(0, half // step, body, 0)


def dot_t(left, right):
    return lax.dot_general(left, right, (((1,), (1,)), ((), ())), preferred_element_type=f32)


def send_terms(at_ref, value_ref, downs, mine_ref, others_ref):
    def body(j, carry):
        for parity, out in ((1, others_ref), (0, mine_ref)):
            at = pl.multiple_of(at_ref[2 * j + parity] * BLK, BLK)
            total = None
            for ref, col, to, width in downs:
                term = dot_t(value_ref[:, to : to + width], ref[pl.ds(at, BLK), col : col + width])
                total = term if total is None else total + term
            out[j] = total.astype(bf16)
        return carry

    lax.fori_loop(0, 4, body, 0)


def half_step_kernel(at_ref, *refs, rows, weights, columns):
    x_refs, gain_ref = refs[0:14], refs[14]
    weight_refs = refs[15 : 15 + weights]
    mine_ref, others_ref, normed_ref, hidden_ref = refs[15 + weights :]
    width = hidden_ref.shape[1]
    (gate_at, gate_col), (up_at, up_col), downs = columns
    norm_into(x_refs, at_ref, gain_ref, normed_ref, rows)
    step = min(512, rows)

    def body(i, carry):
        span = pl.ds(pl.multiple_of(i * step, step), step)
        normed = normed_ref[span, :]
        gate = jnp.dot(
            normed, weight_refs[gate_at][:, gate_col : gate_col + width], preferred_element_type=f32
        )
        up = jnp.dot(normed, weight_refs[up_at][:, up_col : up_col + width], preferred_element_type=f32)
        hidden_ref[span, :] = (gate * jax.nn.sigmoid(gate) * up).astype(bf16)
        return carry

    lax.fori_loop(0, rows // step, body, 0)
    downs = [(weight_refs[r], col, to, w) for r, col, to, w in downs]
    send_terms(at_ref, hidden_ref, downs, mine_ref, others_ref)


def one_minus_exp(value):
    small = jnp.zeros_like(value)
    for n in (8, 7, 6, 5, 4, 3, 2):
        small = value * (1.0 / n) * (1.0 + small)
    small = value * (1.0 + small)
    return jnp.where(value > -0.5, -small, 1.0 - jnp.exp(value))


def shifted(value, by, fill):
    rows = value.shape[0]
    if by % 8 == 0:
        head = jnp.full((by, value.shape[1]), fill, value.dtype)
        return jnp.concatenate([head, value[: rows - by]], axis=0)
    rolled = pltpu.roll(value, by, 0)
    at = lax.broadcasted_iota(jnp.int32, value.shape, 0)
    return jnp.where(at < by, fill, rolled)


def mixer_kernel(at_ref, *refs, rows):
    x_refs = refs[0:14]
    gain_ref, weight_ref, conv_ref, rate_ref, input_ref, slope_ref, shift_ref = refs[14:21]
    mine_ref, others_ref, normed_ref, mixed_ref = refs[21:25]
    width = weight_ref.shape[1] // 3
    norm_into(x_refs, at_ref, gain_ref, normed_ref, rows)
    both = jnp.dot(normed_ref[...], weight_ref[:, : 2 * width], preferred_element_type=f32)
    lane = both[:, :width].astype(bf16).astype(f32)
    branch = both[:, width:]
    conv = lane * conv_ref[CONV - 1].astype(f32)
    for back in range(1, CONV):
        conv = conv + shifted(lane, back, 0.0) * conv_ref[CONV - 1 - back].astype(f32)
    conv = conv.astype(bf16)
    rate = jax.nn.sigmoid(jnp.dot(conv, rate_ref[...], preferred_element_type=f32))
    admit = jax.nn.sigmoid(jnp.dot(conv, input_ref[...], preferred_element_type=f32))
    at = lax.broadcasted_iota(jnp.int32, (rows, width), 1)
    shift = jnp.where(at < HEAD_DIM, shift_ref[:, 0:1], shift_ref[:, 1:2])
    log_decay = rate_scale * rate * slope_ref[...] + shift
    state = jnp.sqrt(one_minus_exp(2.0 * log_decay)) * admit * conv.astype(f32)
    decay = jnp.exp(log_decay)
    by = 1
    while by < rows:
        state = state + decay * shifted(state, by, 0.0)
        if by * 2 < rows:
            decay = decay * shifted(decay, by, 1.0)
        by *= 2
    gelu = jax.nn.gelu(branch)
    mixed_ref[...] = (state * gelu).astype(bf16)
    send_terms(at_ref, mixed_ref, [(weight_ref, 2 * width, 0, width)], mine_ref, others_ref)


def call(kernel, at, operands, rows, width):
    vmem = pl.BlockSpec(memory_space=pltpu.VMEM)
    return pl.pallas_call(
        functools.partial(kernel, rows=rows),
        out_shape=[jax.ShapeDtypeStruct((4, rows, BLK), bf16)] * 2,
        in_specs=[pl.BlockSpec(memory_space=pltpu.SMEM)] + [vmem] * len(operands),
        out_specs=[vmem] * 2,
        scratch_shapes=[pltpu.VMEM((rows, D), bf16), pltpu.VMEM((rows, width), bf16)],
        compiler_params=pltpu.CompilerParams(vmem_limit_bytes=34 * 1024 * 1024),
    )(at, *operands)


def gathered(arrays):
    both = jnp.concatenate(arrays, axis=1)
    return lax.all_gather(both, "fs", axis=0, tiled=True)


def block_map(weight):
    zero = jnp.zeros((HEAD_DIM, HEAD_DIM), weight.dtype)
    return jnp.block([[weight[0], zero], [zero, weight[1]]])


def shards(
    tokens,
    first_gain,
    first_gate,
    first_up,
    first_down,
    mix_gain,
    mix_input,
    mix_branch,
    conv_weight,
    rate_weight,
    input_weight,
    decay_param,
    decay_shift,
    mix_output,
    second_gain,
    second_gate,
    second_up,
    second_down,
    final_gain,
):
    rows = tokens.shape[0]
    at = owners()
    width = first_gate.shape[1]
    cut = 256
    first = gather_rows_by_permute(
        jnp.concatenate([first_gate, first_down[:, :cut]], axis=1),
        jnp.concatenate([first_up, first_down[:, cut:]], axis=1),
    )
    first_columns = ((0, 0), (1, 0), ((0, width, 0, cut), (1, width, cut, width - cut)))
    mix = gathered((mix_input, mix_branch, mix_output))
    second, first = lax.optimization_barrier(
        (jnp.concatenate([second_gate, second_up, second_down], axis=1), first)
    )
    second = (lax.all_gather(second, "fs", axis=0, tiled=True),)
    second_columns = ((0, 0), (0, width), ((0, 2 * width, 0, width),))
    gains = [g.reshape(8, 1, BLK) for g in (first_gain, mix_gain, second_gain)]
    slope = jax.nn.log_sigmoid(decay_param).reshape(1, -1)
    rate_map, input_map = block_map(rate_weight), block_map(input_weight)

    def half(stream, gain, weights, columns):
        blocks = gather_row_blocks(stream)
        kernel = functools.partial(half_step_kernel, weights=len(weights), columns=columns)
        terms = call(kernel, at, (*blocks, gain, *weights), rows, width)
        return stream.astype(f32) + 0.5 * scatter_row_blocks(*terms)

    stream = half(tokens, gains[0], first, first_columns).astype(bf16)
    blocks = gather_row_blocks(stream)
    terms = call(
        mixer_kernel,
        at,
        (*blocks, gains[1], mix, conv_weight, rate_map, input_map, slope, decay_shift),
        rows,
        mix.shape[1] // 3,
    )
    stream = (stream.astype(f32) + scatter_row_blocks(*terms)).astype(bf16)
    values = half(stream, gains[2], second, second_columns).astype(bf16).astype(f32)
    mine = jnp.sum(values * values, axis=1)
    pair = mine + swap(mine)
    square = pair + ring(pair, 1) + ring(pair, -1) + ring(pair, 2)
    scale = lax.rsqrt(square / D + norm_eps)
    return (values * scale[:, None] * final_gain).astype(bf16)


def solution(mesh):
    finer = Mesh(mesh.devices.reshape(mesh.shape["fs"], 4, 2), ("fs", "tp_0", "tp_1"))
    placed = (
        P("fs", TP),
        P(),
        P("fs", TP),
        P("fs", TP),
        P("fs", TP),
        P(),
        P("fs", TP),
        P("fs", TP),
        P(None, TP),
        P(TP, None, None),
        P(TP, None, None),
        P(TP),
        P("fs", TP),
        P("fs", TP),
        P(),
        P("fs", TP),
        P("fs", TP),
        P("fs", TP),
        P(TP),
    )
    return jax.shard_map(
        shards, mesh=finer, in_specs=placed, out_specs=P("fs", TP), check_vma=False
    )
```

```python
import functools

import jax
import jax.numpy as jnp
from jax import lax
from jax.experimental import pallas as pl
from jax.experimental.pallas import tpu as pltpu
from jax.sharding import Mesh
from jax.sharding import PartitionSpec as P


D = 2048
BLK = 256
HEAD_DIM = 64
CONV = 4
TP = ("tp_0", "tp_1")
norm_eps = 1e-06
rate_scale = 8.0
bf16 = jnp.bfloat16
f32 = jnp.float32


OFFSETS = ((0, 0), (0, 1), (1, 0), (1, 1), (-1, 0), (-1, 1), (2, 0), (2, 1))


def ring(value, step):
    return lax.ppermute(value, "tp_0", [(i, (i + step) % 4) for i in range(4)])


def swap(value):
    return lax.ppermute(value, "tp_1", [(0, 1), (1, 0)])


def gather_row_blocks(block):
    half = block.shape[0] // 2
    left = ring(block, 1)
    right = ring(block, -1)
    other = swap(block)
    far_top = ring(left[:half], 1)
    far_low = ring(right[half:], -1)
    right_other, left_other = swap(right), swap(left)
    return (
        block,
        other,
        right,
        right_other,
        left,
        left_other,
        far_top,
        far_low,
        swap(far_top),
        swap(far_low),
    )


def scatter_row_blocks(mine, others):
    half = mine[0].shape[0] // 2
    got = [swap(o) for o in others]
    own, right, left, far = [mine[k].astype(f32) + got[k].astype(f32) for k in range(4)]
    far = far.astype(bf16)
    got_right = ring(far[:half], 1)
    got_left = ring(far[half:], -1)
    right_low = ring(right[half:].astype(bf16), 1)
    left_top = ring(left[:half].astype(bf16), -1)
    right_top = ring((right[:half] + got_right.astype(f32)).astype(bf16), 1)
    left_low = ring((left[half:] + got_left.astype(f32)).astype(bf16), -1)
    top = own[:half] + right_top.astype(f32) + left_top.astype(f32)
    low = own[half:] + right_low.astype(f32) + left_low.astype(f32)
    return jnp.concatenate([top, low], axis=0)


def fs_ring(value, dz, dx):
    pairs = [
        (z * 4 + x, ((z + dz) % 4) * 4 + (x + dx) % 4) for z in range(4) for x in range(4)
    ]
    return lax.ppermute(value, "fs", pairs)


def gather_rows_by_permute(first, second):
    a_line, b_line = [first], [second]
    for step in (1, -1, 2):
        a_line.append(fs_ring(first, 0, step))
        b_line.append(fs_ring(second, step, 0))
    a_line, b_line = jnp.concatenate(a_line, axis=0), jnp.concatenate(b_line, axis=0)
    a_left = fs_ring(a_line, 1, 0)
    a_right = fs_ring(a_line, -1, 0)
    b_left = fs_ring(b_line, 0, 1)
    b_right = fs_ring(b_line, 0, -1)
    half = a_line.shape[0] // 2
    return (
        a_line,
        a_left,
        a_right,
        fs_ring(a_left[:half], 1, 0),
        fs_ring(a_right[half:], -1, 0),
        b_line,
        b_left,
        b_right,
        fs_ring(b_left[:half], 0, 1),
        fs_ring(b_right[half:], 0, -1),
    )


def place_pieces(at_ref, piece_refs, a_ref, b_ref):
    z, x = at_ref[8], at_ref[9]
    rows = a_ref.shape[0] // 16
    steps = (0, -1, 1, 2)
    for ref, pieces, outer, inner, along_z in (
        (a_ref, piece_refs[:5], z, x, True),
        (b_ref, piece_refs[5:], x, z, False),
    ):
        for n, piece in enumerate(pieces):
            far = (outer + steps[min(n, 3)] + 4) % 4
            first = 2 if n == 4 else 0
            for j in range(piece.shape[0] // rows):
                near = (inner + steps[first + j] + 4) % 4
                row = far * 4 + near if along_z else near * 4 + far
                ref[pl.ds(pl.multiple_of(row * rows, rows), rows), :] = piece[
                    j * rows : (j + 1) * rows, :
                ]


def owners():
    y, c = lax.axis_index("tp_0"), lax.axis_index("tp_1")
    fs = lax.axis_index("fs")
    blocks = [((y + dy) % 4) * 2 + (c + dc) % 2 for dy, dc in OFFSETS]
    return jnp.stack([*blocks, fs // 4, fs % 4]).astype(jnp.int32)


def norm_into(x_refs, at_ref, gain_ref, normed_ref, rows):
    half = rows // 2
    step = min(256, half)
    for side in range(2):
        refs = [*x_refs[:6], x_refs[6 + side], x_refs[8 + side]]

        def body(i, carry, side=side, refs=refs):
            near = pl.ds(pl.multiple_of(side * half + i * step, step), step)
            piece = pl.ds(pl.multiple_of(i * step, step), step)
            spans = [near] * 6 + [piece] * 2
            square = None
            for r, span in zip(refs, spans):
                v = r[span, :].astype(f32)
                square = v * v if square is None else square + v * v
            scale = lax.rsqrt(jnp.sum(square, axis=1, keepdims=True) / D + norm_eps)
            for k, (r, span) in enumerate(zip(refs, spans)):
                at = at_ref[k]
                lane = pl.ds(pl.multiple_of(at * BLK, BLK), BLK)
                normed_ref[near, lane] = (r[span, :].astype(f32) * scale * gain_ref[at]).astype(bf16)
            return carry

        lax.fori_loop(0, half // step, body, 0)


def dot_t(left, right):
    return lax.dot_general(left, right, (((1,), (1,)), ((), ())), preferred_element_type=f32)


def send_terms(at_ref, value_ref, downs, outs):
    for k in (7, 3, 5, 1, 6, 2, 4, 0):
        at = pl.multiple_of(at_ref[k] * BLK, BLK)
        total = None
        for ref, col, to, width in downs:
            term = dot_t(value_ref[:, to : to + width], ref[pl.ds(at, BLK), col : col + width])
            total = term if total is None else total + term
        outs[k][...] = total.astype(bf16)


def half_step_kernel(at_ref, *refs, rows, columns, pieces):
    x_refs, gain_ref = refs[0:10], refs[10]
    count = 10 if pieces else 1
    weight_refs = refs[11 : 11 + count]
    outs, (normed_ref, hidden_ref), whole = refs[11 + count : 19 + count], refs[19 + count : 21 + count], refs[21 + count :]
    width = hidden_ref.shape[1]
    (gate_at, gate_col), (up_at, up_col), downs = columns
    if pieces:
        place_pieces(at_ref, weight_refs, *whole)
        weight_refs = whole
    norm_into(x_refs, at_ref, gain_ref, normed_ref, rows)
    step = min(512, rows)

    def body(i, carry):
        span = pl.ds(pl.multiple_of(i * step, step), step)
        normed = normed_ref[span, :]
        gate = jnp.dot(
            normed, weight_refs[gate_at][:, gate_col : gate_col + width], preferred_element_type=f32
        )
        up = jnp.dot(normed, weight_refs[up_at][:, up_col : up_col + width], preferred_element_type=f32)
        hidden_ref[span, :] = (gate * jax.nn.sigmoid(gate) * up).astype(bf16)
        return carry

    lax.fori_loop(0, rows // step, body, 0)
    downs = [(weight_refs[r], col, to, w) for r, col, to, w in downs]
    send_terms(at_ref, hidden_ref, downs, outs)


def one_minus_exp(value):
    small = jnp.zeros_like(value)
    for n in (8, 7, 6, 5, 4, 3, 2):
        small = value * (1.0 / n) * (1.0 + small)
    small = value * (1.0 + small)
    return jnp.where(value > -0.5, -small, 1.0 - jnp.exp(value))


def shifted(value, by, fill):
    rows = value.shape[0]
    if by % 8 == 0:
        head = jnp.full((by, value.shape[1]), fill, value.dtype)
        return jnp.concatenate([head, value[: rows - by]], axis=0)
    rolled = pltpu.roll(value, by, 0)
    at = lax.broadcasted_iota(jnp.int32, value.shape, 0)
    return jnp.where(at < by, fill, rolled)


def mixer_kernel(at_ref, *refs, rows):
    x_refs = refs[0:10]
    gain_ref, weight_ref, conv_ref, rate_ref, input_ref, slope_ref, shift_ref = refs[10:17]
    outs = refs[17:25]
    normed_ref, mixed_ref = refs[25:27]
    width = weight_ref.shape[1] // 3
    norm_into(x_refs, at_ref, gain_ref, normed_ref, rows)
    both = jnp.dot(normed_ref[...], weight_ref[:, : 2 * width], preferred_element_type=f32)
    lane = both[:, :width].astype(bf16).astype(f32)
    branch = both[:, width:]
    conv = lane * conv_ref[CONV - 1].astype(f32)
    for back in range(1, CONV):
        conv = conv + shifted(lane, back, 0.0) * conv_ref[CONV - 1 - back].astype(f32)
    conv = conv.astype(bf16)
    rate = jax.nn.sigmoid(jnp.dot(conv, rate_ref[...], preferred_element_type=f32))
    admit = jax.nn.sigmoid(jnp.dot(conv, input_ref[...], preferred_element_type=f32))
    at = lax.broadcasted_iota(jnp.int32, (rows, width), 1)
    shift = jnp.where(at < HEAD_DIM, shift_ref[:, 0:1], shift_ref[:, 1:2])
    log_decay = rate_scale * rate * slope_ref[...] + shift
    state = jnp.sqrt(one_minus_exp(2.0 * log_decay)) * admit * conv.astype(f32)
    decay = jnp.exp(log_decay)
    by = 1
    while by < rows:
        state = state + decay * shifted(state, by, 0.0)
        if by * 2 < rows:
            decay = decay * shifted(decay, by, 1.0)
        by *= 2
    gelu = jax.nn.gelu(branch)
    mixed_ref[...] = (state * gelu).astype(bf16)
    send_terms(at_ref, mixed_ref, [(weight_ref, 2 * width, 0, width)], outs)


def call(kernel, at, operands, rows, width, whole=()):
    vmem = pl.BlockSpec(memory_space=pltpu.VMEM)
    scratch = [(rows, D), (rows, width), *whole]
    outs = pl.pallas_call(
        functools.partial(kernel, rows=rows),
        out_shape=[jax.ShapeDtypeStruct((rows, BLK), bf16)] * 8,
        in_specs=[pl.BlockSpec(memory_space=pltpu.SMEM)] + [vmem] * len(operands),
        out_specs=[vmem] * 8,
        scratch_shapes=[pltpu.VMEM(shape, bf16) for shape in scratch],
        compiler_params=pltpu.CompilerParams(vmem_limit_bytes=44 * 1024 * 1024),
    )(at, *operands)
    return outs[0::2], outs[1::2]


def block_map(weight):
    zero = jnp.zeros((HEAD_DIM, HEAD_DIM), weight.dtype)
    return jnp.block([[weight[0], zero], [zero, weight[1]]])


def shards(
    tokens,
    first_gain,
    first_gate,
    first_up,
    first_down,
    mix_gain,
    mix_input,
    mix_branch,
    conv_weight,
    rate_weight,
    input_weight,
    decay_param,
    decay_shift,
    mix_output,
    second_gain,
    second_gate,
    second_up,
    second_down,
    final_gain,
):
    rows = tokens.shape[0]
    at = owners()
    width = first_gate.shape[1]
    cut = 256
    first = gather_rows_by_permute(
        jnp.concatenate([first_gate, first_down[:, :cut]], axis=1),
        jnp.concatenate([first_up, first_down[:, cut:]], axis=1),
    )
    first_columns = ((0, 0), (1, 0), ((0, width, 0, cut), (1, width, cut, width - cut)))
    mix = jnp.concatenate([mix_input, mix_branch, mix_output], axis=1)
    second = jnp.concatenate([second_gate, second_up, second_down], axis=1)
    mix, second, first = lax.optimization_barrier((mix, second, first))
    mix = lax.all_gather(mix, "fs", axis=0, tiled=True)
    second = (lax.all_gather(second, "fs", axis=0, tiled=True),)
    second_columns = ((0, 0), (0, width), ((0, 2 * width, 0, width),))
    gains = [g.reshape(8, 1, BLK) for g in (first_gain, mix_gain, second_gain)]
    slope = jax.nn.log_sigmoid(decay_param).reshape(1, -1)
    rate_map, input_map = block_map(rate_weight), block_map(input_weight)

    def half(stream, gain, weights, columns):
        blocks = gather_row_blocks(stream)
        pieces = len(weights) > 1
        kernel = functools.partial(half_step_kernel, columns=columns, pieces=pieces)
        whole = [(D, weights[k].shape[1]) for k in (0, 5)] if pieces else ()
        terms = call(kernel, at, (*blocks, gain, *weights), rows, width, whole)
        return stream.astype(f32) + 0.5 * scatter_row_blocks(*terms)

    stream = half(tokens, gains[0], first, first_columns).astype(bf16)
    blocks = gather_row_blocks(stream)
    terms = call(
        mixer_kernel,
        at,
        (*blocks, gains[1], mix, conv_weight, rate_map, input_map, slope, decay_shift),
        rows,
        mix.shape[1] // 3,
    )
    stream = (stream.astype(f32) + scatter_row_blocks(*terms)).astype(bf16)
    values = half(stream, gains[2], second, second_columns).astype(bf16).astype(f32)
    mine = jnp.sum(values * values, axis=1)
    pair = mine + swap(mine)
    square = pair + ring(pair, 1) + ring(pair, -1) + ring(pair, 2)
    scale = lax.rsqrt(square / D + norm_eps)
    return (values * scale[:, None] * final_gain).astype(bf16)


def solution(mesh):
    finer = Mesh(mesh.devices.reshape(mesh.shape["fs"], 4, 2), ("fs", "tp_0", "tp_1"))
    placed = (
        P("fs", TP),
        P(),
        P("fs", TP),
        P("fs", TP),
        P("fs", TP),
        P(),
        P("fs", TP),
        P("fs", TP),
        P(None, TP),
        P(TP, None, None),
        P(TP, None, None),
        P(TP),
        P("fs", TP),
        P("fs", TP),
        P(),
        P("fs", TP),
        P("fs", TP),
        P("fs", TP),
        P(TP),
    )
    return jax.shard_map(
        shards, mesh=finer, in_specs=placed, out_specs=P("fs", TP), check_vma=False
    )
```

```python
import functools

import jax
import jax.numpy as jnp
from jax import lax
from jax.experimental import pallas as pl
from jax.experimental.pallas import tpu as pltpu
from jax.sharding import Mesh
from jax.sharding import PartitionSpec as P


D = 2048
BLK = 256
HEAD_DIM = 64
CONV = 4
TP = ("tp_0", "tp_1")
norm_eps = 1e-06
rate_scale = 8.0
bf16 = jnp.bfloat16
f32 = jnp.float32


OFFSETS = ((0, 0), (0, 1), (1, 0), (1, 1), (-1, 0), (-1, 1), (2, 0), (2, 1))


def ring(value, step):
    return lax.ppermute(value, "tp_0", [(i, (i + step) % 4) for i in range(4)])


def swap(value):
    return lax.ppermute(value, "tp_1", [(0, 1), (1, 0)])


def gather_row_blocks(block):
    half = block.shape[0] // 2
    left = ring(block, 1)
    right = ring(block, -1)
    other = swap(block)
    far_top = ring(left[:half], 1)
    far_low = ring(right[half:], -1)
    right_other, left_other = swap(right), swap(left)
    return (
        block,
        other,
        right,
        right_other,
        left,
        left_other,
        far_top,
        far_low,
        swap(far_top),
        swap(far_low),
    )


def scatter_row_blocks(mine, others):
    half = mine[0].shape[0] // 2
    got = [swap(others[k]) for k in range(4)]
    own, right, left, far = [mine[k].astype(f32) + got[k].astype(f32) for k in range(4)]
    far = far.astype(bf16)
    got_right = ring(far[:half], 1)
    got_left = ring(far[half:], -1)
    right_low = ring(right[half:].astype(bf16), 1)
    left_top = ring(left[:half].astype(bf16), -1)
    right_top = ring((right[:half] + got_right.astype(f32)).astype(bf16), 1)
    left_low = ring((left[half:] + got_left.astype(f32)).astype(bf16), -1)
    top = own[:half] + right_top.astype(f32) + left_top.astype(f32)
    low = own[half:] + right_low.astype(f32) + left_low.astype(f32)
    return jnp.concatenate([top, low], axis=0)


def fs_ring(value, dz, dx):
    pairs = [
        (z * 4 + x, ((z + dz) % 4) * 4 + (x + dx) % 4) for z in range(4) for x in range(4)
    ]
    return lax.ppermute(value, "fs", pairs)


def gather_rows_by_permute(first, second):
    a_line, b_line = [first], [second]
    for step in (1, -1, 2):
        a_line.append(fs_ring(first, 0, step))
        b_line.append(fs_ring(second, step, 0))
    a_line, b_line = jnp.concatenate(a_line, axis=0), jnp.concatenate(b_line, axis=0)
    a_left = fs_ring(a_line, 1, 0)
    a_right = fs_ring(a_line, -1, 0)
    b_left = fs_ring(b_line, 0, 1)
    b_right = fs_ring(b_line, 0, -1)
    half = a_line.shape[0] // 2
    return (
        a_line,
        a_left,
        a_right,
        fs_ring(a_left[:half], 1, 0),
        fs_ring(a_right[half:], -1, 0),
        b_line,
        b_left,
        b_right,
        fs_ring(b_left[:half], 0, 1),
        fs_ring(b_right[half:], 0, -1),
    )


def piece_copies(at_ref, piece_refs, whole_refs, sems):
    z, x = at_ref[8], at_ref[9]
    rows = whole_refs[0].shape[0] // 16
    steps = (0, -1, 1, 2)
    copies = []
    for ref, pieces, outer, inner, along_z in (
        (whole_refs[0], piece_refs[:5], z, x, True),
        (whole_refs[1], piece_refs[5:], x, z, False),
    ):
        for n, piece in enumerate(pieces):
            far = (outer + steps[min(n, 3)] + 4) % 4
            first = 2 if n == 4 else 0
            for j in range(piece.shape[0] // rows):
                near = (inner + steps[first + j] + 4) % 4
                row = far * 4 + near if along_z else near * 4 + far
                to = ref.at[pl.ds(pl.multiple_of(row * rows, rows), rows), :]
                source = piece.at[pl.ds(j * rows, rows), :]
                copies.append(pltpu.make_async_copy(source, to, sems.at[len(copies)]))
    return copies


def owners():
    y, c = lax.axis_index("tp_0"), lax.axis_index("tp_1")
    fs = lax.axis_index("fs")
    blocks = [((y + dy) % 4) * 2 + (c + dc) % 2 for dy, dc in OFFSETS]
    return jnp.stack([*blocks, fs // 4, fs % 4]).astype(jnp.int32)


def norm_into(x_refs, at_ref, gain_ref, normed_ref, rows):
    half = rows // 2
    step = min(256, half)
    for side in range(2):
        refs = [*x_refs[:6], x_refs[6 + side], x_refs[8 + side]]

        def body(i, carry, side=side, refs=refs):
            near = pl.ds(pl.multiple_of(side * half + i * step, step), step)
            piece = pl.ds(pl.multiple_of(i * step, step), step)
            spans = [near] * 6 + [piece] * 2
            square = None
            for r, span in zip(refs, spans):
                v = r[span, :].astype(f32)
                square = v * v if square is None else square + v * v
            scale = lax.rsqrt(jnp.sum(square, axis=1, keepdims=True) / D + norm_eps)
            for k, (r, span) in enumerate(zip(refs, spans)):
                at = at_ref[k]
                lane = pl.ds(pl.multiple_of(at * BLK, BLK), BLK)
                normed_ref[near, lane] = (r[span, :].astype(f32) * scale * gain_ref[at]).astype(bf16)
            return carry

        lax.fori_loop(0, half // step, body, 0)


def dot_t(left, right):
    return lax.dot_general(left, right, (((1,), (1,)), ((), ())), preferred_element_type=f32)


def send_terms(at_ref, value_ref, downs, mine_ref, others_ref):
    rows = value_ref.shape[0]
    step = min(512, rows)

    def body(j, carry):
        for parity, out in ((1, others_ref), (0, mine_ref)):
            at = pl.multiple_of(at_ref[2 * j + parity] * BLK, BLK)

            def inner(i, carry, at=at, out=out):
                span = pl.ds(pl.multiple_of(i * step, step), step)
                total = None
                for ref, col, to, width in downs:
                    down = ref[pl.ds(at, BLK), col : col + width]
                    term = dot_t(value_ref[span, to : to + width], down)
                    total = term if total is None else total + term
                out[j, span, :] = total.astype(bf16)
                return carry

            lax.fori_loop(0, rows // step, inner, 0)
        return carry

    lax.fori_loop(0, 4, body, 0)


def half_step_kernel(at_ref, *refs, rows, columns, pieces):
    x_refs, gain_ref = refs[0:10], refs[10]
    count = 10 if pieces else 1
    weight_refs = refs[11 : 11 + count]
    mine_ref, others_ref, normed_ref, hidden_ref, sems, *whole = refs[11 + count :]
    width = hidden_ref.shape[1]
    (gate_at, gate_col), (up_at, up_col), downs = columns
    if pieces:
        early, late = piece_copies(at_ref, weight_refs, whole, sems), []
    else:
        parts = [pl.ds(0, 2 * width), pl.ds(2 * width, width)]
        early, late = [
            [pltpu.make_async_copy(weight_refs[0].at[:, p], whole[0].at[:, p], sems.at[k])]
            for k, p in enumerate(parts)
        ]
    for copy in early + late:
        copy.start()
    weight_refs = whole
    norm_into(x_refs, at_ref, gain_ref, normed_ref, rows)
    for copy in early:
        copy.wait()
    step = min(256, rows)

    def body(i, carry):
        span = pl.ds(pl.multiple_of(i * step, step), step)
        normed = normed_ref[span, :]
        gate = jnp.dot(
            normed, weight_refs[gate_at][:, gate_col : gate_col + width], preferred_element_type=f32
        )
        up = jnp.dot(normed, weight_refs[up_at][:, up_col : up_col + width], preferred_element_type=f32)
        hidden_ref[span, :] = (gate * jax.nn.sigmoid(gate) * up).astype(bf16)
        return carry

    lax.fori_loop(0, rows // step, body, 0)
    for copy in late:
        copy.wait()
    downs = [(weight_refs[r], col, to, w) for r, col, to, w in downs]
    send_terms(at_ref, hidden_ref, downs, mine_ref, others_ref)


def join_kernel(gate_ref, up_ref, down_ref, a_ref, b_ref):
    width = gate_ref.shape[1]
    cut = a_ref.shape[1] - width
    a_ref[:, :width] = gate_ref[...]
    a_ref[:, width:] = down_ref[:, :cut]
    b_ref[:, :width] = up_ref[...]
    b_ref[:, width:] = down_ref[:, cut:]


def join_weights(gate, up, down, cut):
    rows, width = gate.shape
    vmem = pl.BlockSpec(memory_space=pltpu.VMEM)
    return pl.pallas_call(
        join_kernel,
        out_shape=[
            jax.ShapeDtypeStruct((rows, width + cut), bf16),
            jax.ShapeDtypeStruct((rows, 2 * width - cut), bf16),
        ],
        in_specs=[vmem] * 3,
        out_specs=[vmem] * 2,
        compiler_params=pltpu.CompilerParams(vmem_limit_bytes=8 * 1024 * 1024),
        name="join",
    )(gate, up, down)


def one_minus_exp(value):
    small = jnp.zeros_like(value)
    for n in (8, 7, 6, 5, 4, 3, 2):
        small = value * (1.0 / n) * (1.0 + small)
    small = value * (1.0 + small)
    return jnp.where(value > -0.5, -small, 1.0 - jnp.exp(value))


def shifted(value, by, fill):
    rows = value.shape[0]
    if by % 8 == 0:
        head = jnp.full((by, value.shape[1]), fill, value.dtype)
        return jnp.concatenate([head, value[: rows - by]], axis=0)
    rolled = pltpu.roll(value, by, 0)
    at = lax.broadcasted_iota(jnp.int32, value.shape, 0)
    return jnp.where(at < by, fill, rolled)


def mixer_kernel(at_ref, *refs, rows):
    x_refs = refs[0:10]
    gain_ref, conv_ref, rate_ref, input_ref, slope_ref, shift_ref, stored_ref = refs[10:17]
    mine_ref, others_ref, normed_ref, mixed_ref, sems, weight_ref, halo_ref, state_ref = refs[17:25]
    width = weight_ref.shape[1] // 3
    copy = pltpu.make_async_copy(stored_ref, weight_ref, sems.at[0])
    copy.start()
    norm_into(x_refs, at_ref, gain_ref, normed_ref, rows)
    copy.wait()
    halo_ref[...] = jnp.zeros_like(halo_ref)
    state_ref[...] = jnp.zeros_like(state_ref)
    step = min(256, rows)

    def body(i, carry):
        span = pl.ds(pl.multiple_of(i * step, step), step)
        both = jnp.dot(normed_ref[span, :], weight_ref[:, : 2 * width], preferred_element_type=f32)
        lane = both[:, :width].astype(bf16).astype(f32)
        before = jnp.concatenate([halo_ref[...], lane], axis=0)
        halo_ref[...] = lane[step - 8 :]
        conv = lane * conv_ref[CONV - 1].astype(f32)
        for back in range(1, CONV):
            conv = conv + before[8 - back : 8 - back + step] * conv_ref[CONV - 1 - back].astype(f32)
        conv = conv.astype(bf16)
        rate = jax.nn.sigmoid(jnp.dot(conv, rate_ref[...], preferred_element_type=f32))
        admit = jax.nn.sigmoid(jnp.dot(conv, input_ref[...], preferred_element_type=f32))
        at = lax.broadcasted_iota(jnp.int32, (step, width), 1)
        shift = jnp.where(at < HEAD_DIM, shift_ref[span, 0:1], shift_ref[span, 1:2])
        log_decay = rate_scale * rate * slope_ref[...] + shift
        state = jnp.sqrt(one_minus_exp(2.0 * log_decay)) * admit * conv.astype(f32)
        decay = jnp.exp(log_decay)
        by = 1
        while by < step:
            state = state + decay * shifted(state, by, 0.0)
            decay = decay * shifted(decay, by, 1.0)
            by *= 2
        state = state + decay * state_ref[7:8, :]
        state_ref[...] = state[step - 8 :]
        mixed_ref[span, :] = (state * jax.nn.gelu(both[:, width:])).astype(bf16)
        return carry

    lax.fori_loop(0, rows // step, body, 0)
    send_terms(at_ref, mixed_ref, [(weight_ref, 2 * width, 0, width)], mine_ref, others_ref)


def call(kernel, at, operands, weights, whole, rows, width, more=(), grant=20):
    vmem = pl.BlockSpec(memory_space=pltpu.VMEM)
    scratch = [
        pltpu.VMEM((rows, D), bf16),
        pltpu.VMEM((rows, width), bf16),
        pltpu.SemaphoreType.DMA((32,)),
        *[pltpu.VMEM(shape, bf16) for shape in whole],
        *more,
    ]
    return pl.pallas_call(
        functools.partial(kernel, rows=rows),
        out_shape=[jax.ShapeDtypeStruct((4, rows, BLK), bf16)] * 2,
        in_specs=[
            pl.BlockSpec(memory_space=pltpu.SMEM),
            *[vmem] * len(operands),
            *[pl.BlockSpec(memory_space=pltpu.HBM)] * len(weights),
        ],
        out_specs=[vmem] * 2,
        scratch_shapes=scratch,
        compiler_params=pltpu.CompilerParams(vmem_limit_bytes=grant * 1024 * 1024),
    )(at, *operands, *[pltpu.with_memory_space_constraint(w, pltpu.HBM) for w in weights])


def block_map(weight):
    zero = jnp.zeros((HEAD_DIM, HEAD_DIM), weight.dtype)
    return jnp.block([[weight[0], zero], [zero, weight[1]]])


def shards(
    tokens,
    first_gain,
    first_gate,
    first_up,
    first_down,
    mix_gain,
    mix_input,
    mix_branch,
    conv_weight,
    rate_weight,
    input_weight,
    decay_param,
    decay_shift,
    mix_output,
    second_gain,
    second_gate,
    second_up,
    second_down,
    final_gain,
):
    rows = tokens.shape[0]
    at = owners()
    width = first_gate.shape[1]
    cut = 256
    first = gather_rows_by_permute(*join_weights(first_gate, first_up, first_down, cut))
    first_columns = ((0, 0), (1, 0), ((0, width, 0, cut), (1, width, cut, width - cut)))
    mix = jnp.concatenate([mix_input, mix_branch, mix_output], axis=1)
    second = jnp.concatenate([second_gate, second_up, second_down], axis=1)
    mix, second, first = lax.optimization_barrier((mix, second, first))
    mix = lax.all_gather(mix, "fs", axis=0, tiled=True)
    second = (lax.all_gather(second, "fs", axis=0, tiled=True),)
    second_columns = ((0, 0), (0, width), ((0, 2 * width, 0, width),))
    gains = [g.reshape(8, 1, BLK) for g in (first_gain, mix_gain, second_gain)]
    slope = jax.nn.log_sigmoid(decay_param).reshape(1, -1)
    rate_map, input_map = block_map(rate_weight), block_map(input_weight)

    def half(stream, gain, weights, columns):
        blocks = gather_row_blocks(stream)
        pieces = len(weights) > 1
        kernel = functools.partial(half_step_kernel, columns=columns, pieces=pieces)
        whole = [(D, w.shape[1]) for w in (weights[0::5] if pieces else weights)]
        terms = call(kernel, at, (*blocks, gain), weights, whole, rows, width)
        return stream.astype(f32) + 0.5 * scatter_row_blocks(*terms)

    stream = half(tokens, gains[0], first, first_columns).astype(bf16)
    blocks = gather_row_blocks(stream)
    terms = call(
        mixer_kernel,
        at,
        (*blocks, gains[1], conv_weight, rate_map, input_map, slope, decay_shift),
        (mix,),
        [mix.shape],
        rows,
        mix.shape[1] // 3,
        [pltpu.VMEM((8, mix.shape[1] // 3), f32)] * 2,
    )
    stream = (stream.astype(f32) + scatter_row_blocks(*terms)).astype(bf16)
    values = half(stream, gains[2], second, second_columns).astype(bf16).astype(f32)
    mine = jnp.sum(values * values, axis=1)
    mine = mine + swap(mine)
    mine = mine + lax.ppermute(mine, "tp_0", [(0, 1), (1, 0), (2, 3), (3, 2)])
    square = mine + lax.ppermute(mine, "tp_0", [(0, 3), (3, 0), (1, 2), (2, 1)])
    scale = lax.rsqrt(square / D + norm_eps)
    return (values * scale[:, None] * final_gain).astype(bf16)


def solution(mesh):
    finer = Mesh(mesh.devices.reshape(mesh.shape["fs"], 4, 2), ("fs", "tp_0", "tp_1"))
    placed = (
        P("fs", TP),
        P(),
        P("fs", TP),
        P("fs", TP),
        P("fs", TP),
        P(),
        P("fs", TP),
        P("fs", TP),
        P(None, TP),
        P(TP, None, None),
        P(TP, None, None),
        P(TP),
        P("fs", TP),
        P("fs", TP),
        P(),
        P("fs", TP),
        P("fs", TP),
        P("fs", TP),
        P(TP),
    )
    return jax.shard_map(
        shards, mesh=finer, in_specs=placed, out_specs=P("fs", TP), check_vma=False
    )
```

```python
import functools

import jax
import jax.numpy as jnp
from jax import lax
from jax.experimental import pallas as pl
from jax.experimental.pallas import tpu as pltpu
from jax.sharding import Mesh
from jax.sharding import PartitionSpec as P


D = 2048
BLK = 256
HEAD_DIM = 64
CONV = 4
TP = ("tp_0", "tp_1")
norm_eps = 1e-06
rate_scale = 8.0
bf16 = jnp.bfloat16
f32 = jnp.float32


OFFSETS = ((0, 0), (0, 1), (1, 0), (1, 1), (-1, 0), (-1, 1), (2, 0), (2, 1))


def ring(value, step):
    return lax.ppermute(value, "tp_0", [(i, (i + step) % 4) for i in range(4)])


def swap(value):
    return lax.ppermute(value, "tp_1", [(0, 1), (1, 0)])


def gather_row_blocks(block):
    half = block.shape[0] // 2
    left = ring(block, 1)
    right = ring(block, -1)
    other = swap(block)
    far_top = ring(left[:half], 1)
    far_low = ring(right[half:], -1)
    right_other, left_other = swap(right), swap(left)
    return (
        block,
        other,
        right,
        right_other,
        left,
        left_other,
        far_top,
        far_low,
        swap(far_top),
        swap(far_low),
    )


def scatter_row_blocks(mine, others):
    half = mine[0].shape[0] // 2
    got = [swap(o) for o in others]
    own, right, left, far = [mine[k].astype(f32) + got[k].astype(f32) for k in range(4)]
    far = far.astype(bf16)
    got_right = ring(far[:half], 1)
    got_left = ring(far[half:], -1)
    right_low = ring(right[half:].astype(bf16), 1)
    left_top = ring(left[:half].astype(bf16), -1)
    right_top = ring((right[:half] + got_right.astype(f32)).astype(bf16), 1)
    left_low = ring((left[half:] + got_left.astype(f32)).astype(bf16), -1)
    top = own[:half] + right_top.astype(f32) + left_top.astype(f32)
    low = own[half:] + right_low.astype(f32) + left_low.astype(f32)
    return jnp.concatenate([top, low], axis=0)


def fs_ring(value, dz, dx):
    pairs = [
        (z * 4 + x, ((z + dz) % 4) * 4 + (x + dx) % 4) for z in range(4) for x in range(4)
    ]
    return lax.ppermute(value, "fs", pairs)


def gather_rows_by_permute(first, second):
    lines = []
    for own, near in ((first, (0, 1)), (second, (1, 0))):
        got = {step: fs_ring(own, step * near[0], step * near[1]) for step in (1, -1, 2)}
        top, low = jnp.concatenate([own, got[1]], axis=0), jnp.concatenate([got[-1], got[2]], axis=0)
        move = lambda v, step: fs_ring(v, step * near[1], step * near[0])
        left_top = move(top, 1)
        right_low = move(low, -1)
        left_low = move(low, 1)
        right_top = move(top, -1)
        far_top = move(left_top, 1)
        far_low = move(right_low, -1)
        lines += [top, low, left_top, left_low, right_top, right_low, far_top, far_low]
    return tuple(lines)


def piece_copies(at_ref, piece_refs, whole_refs, sems):
    z, x = at_ref[8], at_ref[9]
    rows = whole_refs[0].shape[0] // 16
    steps = (0, -1, 1, 2)
    copies = []
    for ref, pieces, outer, inner, along_z in (
        (whole_refs[0], piece_refs[:8], z, x, True),
        (whole_refs[1], piece_refs[8:], x, z, False),
    ):
        for n, piece in enumerate(pieces):
            far = (outer + steps[n // 2] + 4) % 4
            for j in range(2):
                near = (inner + steps[2 * (n % 2) + j] + 4) % 4
                row = far * 4 + near if along_z else near * 4 + far
                to = ref.at[pl.ds(pl.multiple_of(row * rows, rows), rows), :]
                source = piece.at[pl.ds(j * rows, rows), :]
                copies.append(pltpu.make_async_copy(source, to, sems.at[len(copies)]))
    return copies


def owners():
    y, c = lax.axis_index("tp_0"), lax.axis_index("tp_1")
    fs = lax.axis_index("fs")
    blocks = [((y + dy) % 4) * 2 + (c + dc) % 2 for dy, dc in OFFSETS]
    return jnp.stack([*blocks, fs // 4, fs % 4]).astype(jnp.int32)


def norm_into(x_refs, at_ref, gain_ref, normed_ref, rows):
    half = rows // 2
    step = min(256, half)
    for side in range(2):
        refs = [*x_refs[:6], x_refs[6 + side], x_refs[8 + side]]

        def body(i, carry, side=side, refs=refs):
            near = pl.ds(pl.multiple_of(side * half + i * step, step), step)
            piece = pl.ds(pl.multiple_of(i * step, step), step)
            spans = [near] * 6 + [piece] * 2
            square = None
            for r, span in zip(refs, spans):
                v = r[span, :].astype(f32)
                square = v * v if square is None else square + v * v
            scale = lax.rsqrt(jnp.sum(square, axis=1, keepdims=True) / D + norm_eps)
            for k, (r, span) in enumerate(zip(refs, spans)):
                at = at_ref[k]
                lane = pl.ds(pl.multiple_of(at * BLK, BLK), BLK)
                normed_ref[near, lane] = (r[span, :].astype(f32) * scale * gain_ref[at]).astype(bf16)
            return carry

        lax.fori_loop(0, half // step, body, 0)


def dot_t(left, right):
    return lax.dot_general(left, right, (((1,), (1,)), ((), ())), preferred_element_type=f32)


def send_terms(at_ref, value_ref, downs, outs):
    for k in (7, 3, 5, 1, 6, 2, 4, 0):
        at = pl.multiple_of(at_ref[k] * BLK, BLK)
        total = None
        for ref, col, to, width in downs:
            term = dot_t(value_ref[:, to : to + width], ref[pl.ds(at, BLK), col : col + width])
            total = term if total is None else total + term
        outs[k][...] = total.astype(bf16)


def half_step_kernel(at_ref, *refs, rows, columns, pieces):
    x_refs, gain_ref, refs = list(refs[0:10]), refs[10], refs[11:]
    if not pieces:
        stored, x_refs[6:], gain_ref, refs = x_refs[6:], [None] * 4, gain_ref, refs
    count = 16 if pieces else 1
    weight_refs, outs = refs[:count], refs[count : 8 + count]
    normed_ref, hidden_ref, sems, *whole = refs[8 + count :]
    width = hidden_ref.shape[1]
    (gate_at, gate_col), (up_at, up_col), downs = columns
    blocks = []
    if pieces:
        early, late = piece_copies(at_ref, weight_refs, whole, sems), []
    else:
        parts = [pl.ds(0, 2 * width), pl.ds(2 * width, width)]
        early, late = [
            [pltpu.make_async_copy(weight_refs[0].at[:, p], whole[0].at[:, p], sems.at[k])]
            for k, p in enumerate(parts)
        ]
        x_refs[6:] = whole[1:]
        blocks = [
            pltpu.make_async_copy(a, b, sems.at[2 + k])
            for k, (a, b) in enumerate(zip(stored, whole[1:]))
        ]
    for copy in blocks + early + late:
        copy.start()
    weight_refs = whole
    for copy in blocks:
        copy.wait()
    norm_into(x_refs, at_ref, gain_ref, normed_ref, rows)
    for copy in early:
        copy.wait()
    step = min(512, rows)

    def body(i, carry):
        span = pl.ds(pl.multiple_of(i * step, step), step)
        normed = normed_ref[span, :]
        gate = jnp.dot(
            normed, weight_refs[gate_at][:, gate_col : gate_col + width], preferred_element_type=f32
        )
        up = jnp.dot(normed, weight_refs[up_at][:, up_col : up_col + width], preferred_element_type=f32)
        hidden_ref[span, :] = (gate * jax.nn.sigmoid(gate) * up).astype(bf16)
        return carry

    lax.fori_loop(0, rows // step, body, 0)
    for copy in late:
        copy.wait()
    downs = [(weight_refs[r], col, to, w) for r, col, to, w in downs]
    send_terms(at_ref, hidden_ref, downs, outs)


def join_kernel(gate_ref, up_ref, down_ref, a_ref, b_ref, sems):
    width = gate_ref.shape[1]
    cut = a_ref.shape[1] - width
    copies = [
        pltpu.make_async_copy(source, to, sems.at[k])
        for k, (source, to) in enumerate(
            (
                (gate_ref, a_ref.at[:, pl.ds(0, width)]),
                (down_ref.at[:, pl.ds(0, cut)], a_ref.at[:, pl.ds(width, cut)]),
                (up_ref, b_ref.at[:, pl.ds(0, width)]),
                (down_ref.at[:, pl.ds(cut, width - cut)], b_ref.at[:, pl.ds(width, width - cut)]),
            )
        )
    ]
    for copy in copies:
        copy.start()
    for copy in copies:
        copy.wait()


def in_hbm(value):
    return pltpu.with_memory_space_constraint(value, pltpu.HBM)


def join_weights(gate, up, down, cut):
    rows, width = gate.shape
    return pl.pallas_call(
        join_kernel,
        out_shape=[
            jax.ShapeDtypeStruct((rows, width + cut), bf16),
            jax.ShapeDtypeStruct((rows, 2 * width - cut), bf16),
        ],
        in_specs=[pl.BlockSpec(memory_space=pltpu.HBM)] * 3,
        out_specs=[pl.BlockSpec(memory_space=pltpu.VMEM)] * 2,
        scratch_shapes=[pltpu.SemaphoreType.DMA((4,))],
        compiler_params=pltpu.CompilerParams(vmem_limit_bytes=4 * 1024 * 1024),
        name="join",
    )(in_hbm(gate), in_hbm(up), in_hbm(down))


def one_minus_exp(value):
    small = jnp.zeros_like(value)
    for n in (8, 7, 6, 5, 4, 3, 2):
        small = value * (1.0 / n) * (1.0 + small)
    small = value * (1.0 + small)
    return jnp.where(value > -0.5, -small, 1.0 - jnp.exp(value))


def shifted(value, by, fill):
    rows = value.shape[0]
    if by % 8 == 0:
        head = jnp.full((by, value.shape[1]), fill, value.dtype)
        return jnp.concatenate([head, value[: rows - by]], axis=0)
    rolled = pltpu.roll(value, by, 0)
    at = lax.broadcasted_iota(jnp.int32, value.shape, 0)
    return jnp.where(at < by, fill, rolled)


def mixer_kernel(at_ref, *refs, rows):
    x_refs = refs[0:10]
    gain_ref, conv_ref, rate_ref, input_ref, slope_ref, shift_ref, stored_ref = refs[10:17]
    outs = refs[17:25]
    normed_ref, mixed_ref, sems, weight_ref = refs[25:29]
    width = weight_ref.shape[1] // 3
    copy = pltpu.make_async_copy(stored_ref, weight_ref, sems.at[0])
    copy.start()
    norm_into(x_refs, at_ref, gain_ref, normed_ref, rows)
    copy.wait()
    both = jnp.dot(normed_ref[...], weight_ref[:, : 2 * width], preferred_element_type=f32)
    lane = both[:, :width].astype(bf16).astype(f32)
    branch = both[:, width:]
    conv = lane * conv_ref[CONV - 1].astype(f32)
    for back in range(1, CONV):
        conv = conv + shifted(lane, back, 0.0) * conv_ref[CONV - 1 - back].astype(f32)
    conv = conv.astype(bf16)
    rate = jax.nn.sigmoid(jnp.dot(conv, rate_ref[...], preferred_element_type=f32))
    admit = jax.nn.sigmoid(jnp.dot(conv, input_ref[...], preferred_element_type=f32))
    at = lax.broadcasted_iota(jnp.int32, (rows, width), 1)
    shift = jnp.where(at < HEAD_DIM, shift_ref[:, 0:1], shift_ref[:, 1:2])
    log_decay = rate_scale * rate * slope_ref[...] + shift
    state = jnp.sqrt(one_minus_exp(2.0 * log_decay)) * admit * conv.astype(f32)
    decay = jnp.exp(log_decay)
    by = 1
    while by < rows:
        state = state + decay * shifted(state, by, 0.0)
        if by * 2 < rows:
            decay = decay * shifted(decay, by, 1.0)
        by *= 2
    gelu = jax.nn.gelu(branch)
    mixed_ref[...] = (state * gelu).astype(bf16)
    send_terms(at_ref, mixed_ref, [(weight_ref, 2 * width, 0, width)], outs)


def call(kernel, at, operands, stored, whole, rows, width, grant=22):
    vmem, hbm = pl.BlockSpec(memory_space=pltpu.VMEM), pl.BlockSpec(memory_space=pltpu.HBM)
    scratch = [
        pltpu.VMEM((rows, D), bf16),
        pltpu.VMEM((rows, width), bf16),
        pltpu.SemaphoreType.DMA((32,)),
        *[pltpu.VMEM(shape, bf16) for shape in whole],
    ]
    outs = pl.pallas_call(
        functools.partial(kernel, rows=rows),
        out_shape=[jax.ShapeDtypeStruct((rows, BLK), bf16)] * 8,
        in_specs=[
            pl.BlockSpec(memory_space=pltpu.SMEM),
            *[hbm if k in stored else vmem for k in range(len(operands))],
        ],
        out_specs=[vmem] * 8,
        scratch_shapes=scratch,
        compiler_params=pltpu.CompilerParams(vmem_limit_bytes=grant * 1024 * 1024),
    )(at, *[in_hbm(v) if k in stored else v for k, v in enumerate(operands)])
    return outs[0::2], outs[1::2]


def block_map(weight):
    zero = jnp.zeros((HEAD_DIM, HEAD_DIM), weight.dtype)
    return jnp.block([[weight[0], zero], [zero, weight[1]]])


def shards(
    tokens,
    first_gain,
    first_gate,
    first_up,
    first_down,
    mix_gain,
    mix_input,
    mix_branch,
    conv_weight,
    rate_weight,
    input_weight,
    decay_param,
    decay_shift,
    mix_output,
    second_gain,
    second_gate,
    second_up,
    second_down,
    final_gain,
):
    rows = tokens.shape[0]
    at = owners()
    width = first_gate.shape[1]
    cut = 384
    first = gather_rows_by_permute(*join_weights(first_gate, first_up, first_down, cut))
    first_columns = ((0, 0), (1, 0), ((0, width, 0, cut), (1, width, cut, width - cut)))
    mix = jnp.concatenate([mix_input, mix_branch, mix_output], axis=1)
    second = jnp.concatenate([second_gate, second_up, second_down], axis=1)
    mix, second, first = lax.optimization_barrier((mix, second, first))
    mix = lax.all_gather(mix, "fs", axis=0, tiled=True)
    second = (lax.all_gather(second, "fs", axis=0, tiled=True),)
    second_columns = ((0, 0), (0, width), ((0, 2 * width, 0, width),))
    gains = [g.reshape(8, 1, BLK) for g in (first_gain, mix_gain, second_gain)]
    slope = jax.nn.log_sigmoid(decay_param).reshape(1, -1)
    rate_map, input_map = block_map(rate_weight), block_map(input_weight)

    def half(stream, gain, weights, columns):
        blocks = gather_row_blocks(stream)
        pieces = len(weights) > 1
        kernel = functools.partial(half_step_kernel, columns=columns, pieces=pieces)
        operands = (*blocks, gain, *weights)
        whole = [(D, w.shape[1]) for w in (weights[0::8] if pieces else weights)]
        stored = list(range(11, len(operands)))
        if not pieces:
            stored += range(6, 10)
            whole += [b.shape for b in blocks[6:]]
        terms = call(kernel, at, operands, stored, whole, rows, width)
        return stream.astype(f32) + 0.5 * scatter_row_blocks(*terms)

    stream = half(tokens, gains[0], first, first_columns).astype(bf16)
    blocks = gather_row_blocks(stream)
    terms = call(
        mixer_kernel,
        at,
        (*blocks, gains[1], conv_weight, rate_map, input_map, slope, decay_shift, mix),
        [16],
        [mix.shape],
        rows,
        mix.shape[1] // 3,
    )
    stream = (stream.astype(f32) + scatter_row_blocks(*terms)).astype(bf16)
    values = half(stream, gains[2], second, second_columns).astype(bf16).astype(f32)
    mine = jnp.sum(values * values, axis=1)
    mine = mine + swap(mine)
    mine = mine + lax.ppermute(mine, "tp_0", [(0, 1), (1, 0), (2, 3), (3, 2)])
    square = mine + lax.ppermute(mine, "tp_0", [(0, 3), (3, 0), (1, 2), (2, 1)])
    scale = lax.rsqrt(square / D + norm_eps)
    return (values * scale[:, None] * final_gain).astype(bf16)


def solution(mesh):
    finer = Mesh(mesh.devices.reshape(mesh.shape["fs"], 4, 2), ("fs", "tp_0", "tp_1"))
    placed = (
        P("fs", TP),
        P(),
        P("fs", TP),
        P("fs", TP),
        P("fs", TP),
        P(),
        P("fs", TP),
        P("fs", TP),
        P(None, TP),
        P(TP, None, None),
        P(TP, None, None),
        P(TP),
        P("fs", TP),
        P("fs", TP),
        P(),
        P("fs", TP),
        P("fs", TP),
        P("fs", TP),
        P(TP),
    )
    return jax.shard_map(
        shards, mesh=finer, in_specs=placed, out_specs=P("fs", TP), check_vma=False
    )
```

```python
import functools

import jax
import jax.numpy as jnp
from jax import lax
from jax.experimental import pallas as pl
from jax.experimental.pallas import tpu as pltpu
from jax.sharding import Mesh
from jax.sharding import PartitionSpec as P


D = 2048
BLK = 256
HEAD_DIM = 64
CONV = 4
TP = ("tp_0", "tp_1")
norm_eps = 1e-06
rate_scale = 8.0
bf16 = jnp.bfloat16
f32 = jnp.float32


OFFSETS = ((0, 0), (0, 1), (1, 0), (1, 1), (-1, 0), (-1, 1), (2, 0), (2, 1))


def ring(value, step):
    return lax.ppermute(value, "tp_0", [(i, (i + step) % 4) for i in range(4)])


def swap(value):
    return lax.ppermute(value, "tp_1", [(0, 1), (1, 0)])


def gather_row_blocks(block):
    half = block.shape[0] // 2
    left = ring(block, 1)
    right = ring(block, -1)
    other = swap(block)
    far_top = ring(left[:half], 1)
    far_low = ring(right[half:], -1)
    right_other, left_other = swap(right), swap(left)
    return (
        block,
        other,
        right,
        right_other,
        left,
        left_other,
        far_top,
        far_low,
        swap(far_top),
        swap(far_low),
    )


def scatter_row_blocks(mine, others):
    half = mine[0].shape[0] // 2
    got = [swap(o) for o in others]
    own, right, left, far = [mine[k].astype(f32) + got[k].astype(f32) for k in range(4)]
    far = far.astype(bf16)
    got_right = ring(far[:half], 1)
    got_left = ring(far[half:], -1)
    right_low = ring(right[half:].astype(bf16), 1)
    left_top = ring(left[:half].astype(bf16), -1)
    right_top = ring((right[:half] + got_right.astype(f32)).astype(bf16), 1)
    left_low = ring((left[half:] + got_left.astype(f32)).astype(bf16), -1)
    top = own[:half] + right_top.astype(f32) + left_top.astype(f32)
    low = own[half:] + right_low.astype(f32) + left_low.astype(f32)
    return jnp.concatenate([top, low], axis=0)


def fs_ring(value, dz, dx):
    pairs = [
        (z * 4 + x, ((z + dz) % 4) * 4 + (x + dx) % 4) for z in range(4) for x in range(4)
    ]
    return lax.ppermute(value, "fs", pairs)


def gather_rows_by_permute(first, second):
    lines = []
    for own, near in ((first, (0, 1)), (second, (1, 0))):
        got = {step: fs_ring(own, step * near[0], step * near[1]) for step in (1, -1, 2)}
        top, low = jnp.concatenate([own, got[1]], axis=0), jnp.concatenate([got[-1], got[2]], axis=0)
        move = lambda v, step: fs_ring(v, step * near[1], step * near[0])
        left_top = move(top, 1)
        right_low = move(low, -1)
        left_low = move(low, 1)
        right_top = move(top, -1)
        far_top = move(left_top, 1)
        far_low = move(right_low, -1)
        lines += [top, low, left_top, left_low, right_top, right_low, far_top, far_low]
    return tuple(lines)


def piece_copies(at_ref, piece_refs, whole_refs, sems):
    z, x = at_ref[8], at_ref[9]
    rows = whole_refs[0].shape[0] // 16
    steps = (0, -1, 1, 2)
    copies = []
    for ref, pieces, outer, inner, along_z in (
        (whole_refs[0], piece_refs[:8], z, x, True),
        (whole_refs[1], piece_refs[8:], x, z, False),
    ):
        for n, piece in enumerate(pieces):
            far = (outer + steps[n // 2] + 4) % 4
            for j in range(2):
                near = (inner + steps[2 * (n % 2) + j] + 4) % 4
                row = far * 4 + near if along_z else near * 4 + far
                to = ref.at[pl.ds(pl.multiple_of(row * rows, rows), rows), :]
                source = piece.at[pl.ds(j * rows, rows), :]
                copies.append(pltpu.make_async_copy(source, to, sems.at[len(copies)]))
    return copies


def owners():
    y, c = lax.axis_index("tp_0"), lax.axis_index("tp_1")
    fs = lax.axis_index("fs")
    blocks = [((y + dy) % 4) * 2 + (c + dc) % 2 for dy, dc in OFFSETS]
    return jnp.stack([*blocks, fs // 4, fs % 4]).astype(jnp.int32)


def norm_into(x_refs, at_ref, gain_ref, normed_ref, rows):
    half = rows // 2
    step = min(256, half)
    for side in range(2):
        refs = [*x_refs[:6], x_refs[6 + side], x_refs[8 + side]]

        def body(i, carry, side=side, refs=refs):
            near = pl.ds(pl.multiple_of(side * half + i * step, step), step)
            piece = pl.ds(pl.multiple_of(i * step, step), step)
            spans = [near] * 6 + [piece] * 2
            square = None
            for r, span in zip(refs, spans):
                v = r[span, :].astype(f32)
                square = v * v if square is None else square + v * v
            scale = lax.rsqrt(jnp.sum(square, axis=1, keepdims=True) / D + norm_eps)
            for k, (r, span) in enumerate(zip(refs, spans)):
                at = at_ref[k]
                lane = pl.ds(pl.multiple_of(at * BLK, BLK), BLK)
                normed_ref[near, lane] = (r[span, :].astype(f32) * scale * gain_ref[at]).astype(bf16)
            return carry

        lax.fori_loop(0, half // step, body, 0)


def dot_t(left, right):
    return lax.dot_general(left, right, (((1,), (1,)), ((), ())), preferred_element_type=f32)


def send_terms(at_ref, value_ref, downs, outs):
    for k in (7, 3, 5, 1, 6, 2, 4, 0):
        at = pl.multiple_of(at_ref[k] * BLK, BLK)
        total = None
        for ref, col, to, width in downs:
            term = dot_t(value_ref[:, to : to + width], ref[pl.ds(at, BLK), col : col + width])
            total = term if total is None else total + term
        outs[k][...] = total.astype(bf16)


def half_step_kernel(at_ref, *refs, rows, columns, pieces):
    x_refs, gain_ref, refs = list(refs[0:10]), refs[10], refs[11:]
    if not pieces:
        stored, x_refs[6:], gain_ref, refs = x_refs[6:], [None] * 4, gain_ref, refs
    count = 16 if pieces else 1
    weight_refs, outs = refs[:count], refs[count : 8 + count]
    normed_ref, hidden_ref, sems, *whole = refs[8 + count :]
    width = hidden_ref.shape[1]
    (gate_at, gate_col), (up_at, up_col), downs = columns
    if pieces:
        early, late = piece_copies(at_ref, weight_refs, whole, sems), []
        blocks = [pltpu.make_async_copy(x_refs[0], whole[2], sems.at[32])]
        x_refs[0] = whole[2]
    else:
        parts = [pl.ds(0, 2 * width), pl.ds(2 * width, width)]
        early, late = [
            [pltpu.make_async_copy(weight_refs[0].at[:, p], whole[0].at[:, p], sems.at[k])]
            for k, p in enumerate(parts)
        ]
        x_refs[6:] = whole[1:]
        blocks = [
            pltpu.make_async_copy(a, b, sems.at[2 + k])
            for k, (a, b) in enumerate(zip(stored, whole[1:]))
        ]
    for copy in blocks + early + late:
        copy.start()
    weight_refs = whole
    for copy in blocks:
        copy.wait()
    norm_into(x_refs, at_ref, gain_ref, normed_ref, rows)
    for copy in early:
        copy.wait()
    step = min(512, rows)

    def body(i, carry):
        span = pl.ds(pl.multiple_of(i * step, step), step)
        normed = normed_ref[span, :]
        gate = jnp.dot(
            normed, weight_refs[gate_at][:, gate_col : gate_col + width], preferred_element_type=f32
        )
        up = jnp.dot(normed, weight_refs[up_at][:, up_col : up_col + width], preferred_element_type=f32)
        hidden_ref[span, :] = (gate * jax.nn.sigmoid(gate) * up).astype(bf16)
        return carry

    lax.fori_loop(0, rows // step, body, 0)
    for copy in late:
        copy.wait()
    downs = [(weight_refs[r], col, to, w) for r, col, to, w in downs]
    send_terms(at_ref, hidden_ref, downs, outs)


def join_kernel(gate_ref, up_ref, down_ref, a_ref, b_ref, sems):
    width = gate_ref.shape[1]
    cut = a_ref.shape[1] - width
    copies = [
        pltpu.make_async_copy(source, to, sems.at[k])
        for k, (source, to) in enumerate(
            (
                (gate_ref, a_ref.at[:, pl.ds(0, width)]),
                (down_ref.at[:, pl.ds(0, cut)], a_ref.at[:, pl.ds(width, cut)]),
                (up_ref, b_ref.at[:, pl.ds(0, width)]),
                (down_ref.at[:, pl.ds(cut, width - cut)], b_ref.at[:, pl.ds(width, width - cut)]),
            )
        )
    ]
    for copy in copies:
        copy.start()
    for copy in copies:
        copy.wait()


def in_hbm(value):
    return pltpu.with_memory_space_constraint(value, pltpu.HBM)


def join_weights(gate, up, down, cut):
    rows, width = gate.shape
    return pl.pallas_call(
        join_kernel,
        out_shape=[
            jax.ShapeDtypeStruct((rows, width + cut), bf16),
            jax.ShapeDtypeStruct((rows, 2 * width - cut), bf16),
        ],
        in_specs=[pl.BlockSpec(memory_space=pltpu.HBM)] * 3,
        out_specs=[pl.BlockSpec(memory_space=pltpu.VMEM)] * 2,
        scratch_shapes=[pltpu.SemaphoreType.DMA((4,))],
        compiler_params=pltpu.CompilerParams(vmem_limit_bytes=4 * 1024 * 1024),
        name="join",
    )(in_hbm(gate), in_hbm(up), in_hbm(down))


def one_minus_exp(value):
    small = jnp.zeros_like(value)
    for n in (8, 7, 6, 5, 4, 3, 2):
        small = value * (1.0 / n) * (1.0 + small)
    small = value * (1.0 + small)
    return jnp.where(value > -0.5, -small, 1.0 - jnp.exp(value))


def shifted(value, by, fill):
    rows = value.shape[0]
    if by % 8 == 0:
        head = jnp.full((by, value.shape[1]), fill, value.dtype)
        return jnp.concatenate([head, value[: rows - by]], axis=0)
    rolled = pltpu.roll(value, by, 0)
    at = lax.broadcasted_iota(jnp.int32, value.shape, 0)
    return jnp.where(at < by, fill, rolled)


def mixer_kernel(at_ref, *refs, rows):
    x_refs = refs[0:10]
    gain_ref, conv_ref, rate_ref, input_ref, slope_ref, shift_ref, stored_ref = refs[10:17]
    outs = refs[17:25]
    normed_ref, mixed_ref, sems, weight_ref = refs[25:29]
    width = weight_ref.shape[1] // 3
    copy = pltpu.make_async_copy(stored_ref, weight_ref, sems.at[0])
    copy.start()
    norm_into(x_refs, at_ref, gain_ref, normed_ref, rows)
    copy.wait()
    both = jnp.dot(normed_ref[...], weight_ref[:, : 2 * width], preferred_element_type=f32)
    lane = both[:, :width].astype(bf16).astype(f32)
    branch = both[:, width:]
    conv = lane * conv_ref[CONV - 1].astype(f32)
    for back in range(1, CONV):
        conv = conv + shifted(lane, back, 0.0) * conv_ref[CONV - 1 - back].astype(f32)
    conv = conv.astype(bf16)
    rate = jax.nn.sigmoid(jnp.dot(conv, rate_ref[...], preferred_element_type=f32))
    admit = jax.nn.sigmoid(jnp.dot(conv, input_ref[...], preferred_element_type=f32))
    at = lax.broadcasted_iota(jnp.int32, (rows, width), 1)
    shift = jnp.where(at < HEAD_DIM, shift_ref[:, 0:1], shift_ref[:, 1:2])
    log_decay = rate_scale * rate * slope_ref[...] + shift
    state = jnp.sqrt(one_minus_exp(2.0 * log_decay)) * admit * conv.astype(f32)
    decay = jnp.exp(log_decay)
    by = 1
    while by < rows:
        state = state + decay * shifted(state, by, 0.0)
        if by * 2 < rows:
            decay = decay * shifted(decay, by, 1.0)
        by *= 2
    gelu = jax.nn.gelu(branch)
    mixed_ref[...] = (state * gelu).astype(bf16)
    send_terms(at_ref, mixed_ref, [(weight_ref, 2 * width, 0, width)], outs)


def call(kernel, at, operands, stored, whole, rows, width, grant=22):
    vmem, hbm = pl.BlockSpec(memory_space=pltpu.VMEM), pl.BlockSpec(memory_space=pltpu.HBM)
    scratch = [
        pltpu.VMEM((rows, D), bf16),
        pltpu.VMEM((rows, width), bf16),
        pltpu.SemaphoreType.DMA((33,)),
        *[pltpu.VMEM(shape, bf16) for shape in whole],
    ]
    outs = pl.pallas_call(
        functools.partial(kernel, rows=rows),
        out_shape=[jax.ShapeDtypeStruct((rows, BLK), bf16)] * 8,
        in_specs=[
            pl.BlockSpec(memory_space=pltpu.SMEM),
            *[hbm if k in stored else vmem for k in range(len(operands))],
        ],
        out_specs=[vmem] * 8,
        scratch_shapes=scratch,
        compiler_params=pltpu.CompilerParams(vmem_limit_bytes=grant * 1024 * 1024),
    )(at, *[in_hbm(v) if k in stored else v for k, v in enumerate(operands)])
    return outs[0::2], outs[1::2]


def block_map(weight):
    zero = jnp.zeros((HEAD_DIM, HEAD_DIM), weight.dtype)
    return jnp.block([[weight[0], zero], [zero, weight[1]]])


def shards(
    tokens,
    first_gain,
    first_gate,
    first_up,
    first_down,
    mix_gain,
    mix_input,
    mix_branch,
    conv_weight,
    rate_weight,
    input_weight,
    decay_param,
    decay_shift,
    mix_output,
    second_gain,
    second_gate,
    second_up,
    second_down,
    final_gain,
):
    rows = tokens.shape[0]
    at = owners()
    width = first_gate.shape[1]
    cut = 384
    first = gather_rows_by_permute(*join_weights(first_gate, first_up, first_down, cut))
    first_columns = ((0, 0), (1, 0), ((0, width, 0, cut), (1, width, cut, width - cut)))
    mix = jnp.concatenate([mix_input, mix_branch, mix_output], axis=1)
    second = jnp.concatenate([second_gate, second_up, second_down], axis=1)
    mix, second, first = lax.optimization_barrier((mix, second, first))
    mix = lax.all_gather(mix, "fs", axis=0, tiled=True)
    second = (lax.all_gather(second, "fs", axis=0, tiled=True),)
    second_columns = ((0, 0), (0, width), ((0, 2 * width, 0, width),))
    gains = [g.reshape(8, 1, BLK) for g in (first_gain, mix_gain, second_gain)]
    slope = jax.nn.log_sigmoid(decay_param).reshape(1, -1)
    rate_map, input_map = block_map(rate_weight), block_map(input_weight)

    def half(stream, gain, weights, columns):
        blocks = gather_row_blocks(stream)
        pieces = len(weights) > 1
        kernel = functools.partial(half_step_kernel, columns=columns, pieces=pieces)
        operands = (*blocks, gain, *weights)
        whole = [(D, w.shape[1]) for w in (weights[0::8] if pieces else weights)]
        stored = list(range(11, len(operands)))
        kept = range(1) if pieces else range(6, 10)
        stored += kept
        whole += [blocks[k].shape for k in kept]
        terms = call(kernel, at, operands, stored, whole, rows, width)
        return stream.astype(f32) + 0.5 * scatter_row_blocks(*terms)

    stream = half(tokens, gains[0], first, first_columns).astype(bf16)
    blocks = gather_row_blocks(stream)
    terms = call(
        mixer_kernel,
        at,
        (*blocks, gains[1], conv_weight, rate_map, input_map, slope, decay_shift, mix),
        [16],
        [mix.shape],
        rows,
        mix.shape[1] // 3,
    )
    stream = (stream.astype(f32) + scatter_row_blocks(*terms)).astype(bf16)
    values = half(stream, gains[2], second, second_columns).astype(bf16).astype(f32)
    mine = jnp.sum(values * values, axis=1)
    mine = mine + swap(mine)
    mine = mine + lax.ppermute(mine, "tp_0", [(0, 1), (1, 0), (2, 3), (3, 2)])
    square = mine + lax.ppermute(mine, "tp_0", [(0, 3), (3, 0), (1, 2), (2, 1)])
    scale = lax.rsqrt(square / D + norm_eps)
    return (values * scale[:, None] * final_gain).astype(bf16)


def solution(mesh):
    finer = Mesh(mesh.devices.reshape(mesh.shape["fs"], 4, 2), ("fs", "tp_0", "tp_1"))
    placed = (
        P("fs", TP),
        P(),
        P("fs", TP),
        P("fs", TP),
        P("fs", TP),
        P(),
        P("fs", TP),
        P("fs", TP),
        P(None, TP),
        P(TP, None, None),
        P(TP, None, None),
        P(TP),
        P("fs", TP),
        P("fs", TP),
        P(),
        P("fs", TP),
        P("fs", TP),
        P("fs", TP),
        P(TP),
    )
    return jax.shard_map(
        shards, mesh=finer, in_specs=placed, out_specs=P("fs", TP), check_vma=False
    )
```

```python
import functools

import jax
import jax.numpy as jnp
from jax import lax
from jax.experimental import pallas as pl
from jax.experimental.pallas import tpu as pltpu
from jax.sharding import Mesh
from jax.sharding import PartitionSpec as P


D = 2048
BLK = 256
HEAD_DIM = 64
CONV = 4
TP = ("tp_0", "tp_1")
norm_eps = 1e-06
rate_scale = 8.0
bf16 = jnp.bfloat16
f32 = jnp.float32


OFFSETS = ((0, 0), (0, 1), (1, 0), (1, 1), (-1, 0), (-1, 1), (2, 0), (2, 1))


def ring(value, step):
    return lax.ppermute(value, "tp_0", [(i, (i + step) % 4) for i in range(4)])


def swap(value):
    return lax.ppermute(value, "tp_1", [(0, 1), (1, 0)])


def gather_row_blocks(block):
    half = block.shape[0] // 2
    left = ring(block, 1)
    right = ring(block, -1)
    other = swap(block)
    far_top = ring(left[:half], 1)
    far_low = ring(right[half:], -1)
    right_other, left_other = swap(right), swap(left)
    return (block, other, right, right_other, left, left_other, far_top, far_low, swap(far_top), swap(far_low))


def gather_row_halves(block):
    half = block.shape[0] // 2
    top, low = block[:half], block[half:]
    left_top = ring(top, 1)
    right_low = ring(low, -1)
    left_low = ring(low, 1)
    right_top = ring(top, -1)
    other = swap(block)
    far_top = ring(left_top, 1)
    far_low = ring(right_low, -1)
    pairs = (right_top, right_low), (left_top, left_low), (far_top, far_low)
    blocks = [block, other]
    for pair in pairs:
        blocks += [*pair, *[swap(h) for h in pair]]
    return tuple(blocks)


WHOLE_PARTS = (1, 1, 1, 1, 1, 1, 2, 2)
HALF_PARTS = (1, 1, 2, 2, 2, 2, 2, 2)


def scatter_row_blocks(mine, others):
    half = mine[0].shape[0] // 2
    got = [swap(o) for o in others]
    own, right, left, far = [mine[k].astype(f32) + got[k].astype(f32) for k in range(4)]
    far = far.astype(bf16)
    got_right = ring(far[:half], 1)
    got_left = ring(far[half:], -1)
    right_low = ring(right[half:].astype(bf16), 1)
    left_top = ring(left[:half].astype(bf16), -1)
    right_top = ring((right[:half] + got_right.astype(f32)).astype(bf16), 1)
    left_low = ring((left[half:] + got_left.astype(f32)).astype(bf16), -1)
    top = own[:half] + right_top.astype(f32) + left_top.astype(f32)
    low = own[half:] + right_low.astype(f32) + left_low.astype(f32)
    return jnp.concatenate([top, low], axis=0)


def fs_ring(value, dz, dx):
    pairs = [
        (z * 4 + x, ((z + dz) % 4) * 4 + (x + dx) % 4) for z in range(4) for x in range(4)
    ]
    return lax.ppermute(value, "fs", pairs)


def gather_rows_by_permute(first, second):
    lines = []
    for own, near in ((first, (0, 1)), (second, (1, 0))):
        got = {step: fs_ring(own, step * near[0], step * near[1]) for step in (1, -1, 2)}
        top, low = jnp.concatenate([own, got[1]], axis=0), jnp.concatenate([got[-1], got[2]], axis=0)
        move = lambda v, step: fs_ring(v, step * near[1], step * near[0])
        left_top = move(top, 1)
        right_low = move(low, -1)
        left_low = move(low, 1)
        right_top = move(top, -1)
        far_top = move(left_top, 1)
        far_low = move(right_low, -1)
        lines += [top, low, left_top, left_low, right_top, right_low, far_top, far_low]
    return tuple(lines)


def piece_copies(at_ref, piece_refs, whole_refs, sems):
    z, x = at_ref[8], at_ref[9]
    rows = whole_refs[0].shape[0] // 16
    steps = (0, -1, 1, 2)
    copies = []
    for ref, pieces, outer, inner, along_z in (
        (whole_refs[0], piece_refs[:8], z, x, True),
        (whole_refs[1], piece_refs[8:], x, z, False),
    ):
        for n, piece in enumerate(pieces):
            far = (outer + steps[n // 2] + 4) % 4
            for j in range(2):
                near = (inner + steps[2 * (n % 2) + j] + 4) % 4
                row = far * 4 + near if along_z else near * 4 + far
                to = ref.at[pl.ds(pl.multiple_of(row * rows, rows), rows), :]
                source = piece.at[pl.ds(j * rows, rows), :]
                copies.append(pltpu.make_async_copy(source, to, sems.at[len(copies)]))
    return copies


def owners():
    y, c = lax.axis_index("tp_0"), lax.axis_index("tp_1")
    fs = lax.axis_index("fs")
    blocks = [((y + dy) % 4) * 2 + (c + dc) % 2 for dy, dc in OFFSETS]
    return jnp.stack([*blocks, fs // 4, fs % 4]).astype(jnp.int32)


def norm_into(x_refs, parts, at_ref, gain_ref, normed_ref, rows):
    half = rows // 2
    step = min(256, half)
    starts = [sum(parts[:k]) for k in range(8)]
    for side in range(2):
        refs = [x_refs[at + side * (n - 1)] for at, n in zip(starts, parts)]

        def body(i, carry, side=side, refs=refs):
            near = pl.ds(pl.multiple_of(side * half + i * step, step), step)
            piece = pl.ds(pl.multiple_of(i * step, step), step)
            spans = [near if n == 1 else piece for n in parts]
            square = None
            for r, span in zip(refs, spans):
                v = r[span, :].astype(f32)
                square = v * v if square is None else square + v * v
            scale = lax.rsqrt(jnp.sum(square, axis=1, keepdims=True) / D + norm_eps)
            for k, (r, span) in enumerate(zip(refs, spans)):
                at = at_ref[k]
                lane = pl.ds(pl.multiple_of(at * BLK, BLK), BLK)
                normed_ref[near, lane] = (r[span, :].astype(f32) * scale * gain_ref[at]).astype(bf16)
            return carry

        lax.fori_loop(0, half // step, body, 0)


def dot_t(left, right):
    return lax.dot_general(left, right, (((1,), (1,)), ((), ())), preferred_element_type=f32)


def send_terms(at_ref, value_ref, downs, outs):
    for k in (7, 3, 5, 1, 6, 2, 4, 0):
        at = pl.multiple_of(at_ref[k] * BLK, BLK)
        total = None
        for ref, col, to, width in downs:
            term = dot_t(value_ref[:, to : to + width], ref[pl.ds(at, BLK), col : col + width])
            total = term if total is None else total + term
        outs[k][...] = total.astype(bf16)


def half_step_kernel(at_ref, *refs, rows, columns, pieces, parts, stored):
    blocks = sum(parts)
    x_refs, gain_ref, refs = list(refs[:blocks]), refs[blocks], refs[blocks + 1 :]
    count = 16 if pieces else 1
    weight_refs, outs = refs[:count], refs[count : 8 + count]
    normed_ref, hidden_ref, sems, *whole = refs[8 + count :]
    whole, kept_gain, kept = whole[: 1 + pieces], whole[1 + pieces], whole[2 + pieces :]
    width = hidden_ref.shape[1]
    (gate_at, gate_col), (up_at, up_col), downs = columns
    first = [pltpu.make_async_copy(gain_ref, kept_gain, sems.at[32])]
    for n, k in enumerate(stored):
        first.append(pltpu.make_async_copy(x_refs[k], kept[n], sems.at[33 + n]))
        x_refs[k] = kept[n]
    if pieces:
        early, late = piece_copies(at_ref, weight_refs, whole, sems), []
    else:
        spans = [pl.ds(0, 2 * width), pl.ds(2 * width, width)]
        early, late = [
            [pltpu.make_async_copy(weight_refs[0].at[:, p], whole[0].at[:, p], sems.at[k])]
            for k, p in enumerate(spans)
        ]
    for copy in first + early + late:
        copy.start()
    weight_refs = whole
    for copy in first:
        copy.wait()
    norm_into(x_refs, parts, at_ref, kept_gain, normed_ref, rows)
    for copy in early:
        copy.wait()
    step = min(512, rows)

    def body(i, carry):
        span = pl.ds(pl.multiple_of(i * step, step), step)
        normed = normed_ref[span, :]
        gate = jnp.dot(
            normed, weight_refs[gate_at][:, gate_col : gate_col + width], preferred_element_type=f32
        )
        up = jnp.dot(normed, weight_refs[up_at][:, up_col : up_col + width], preferred_element_type=f32)
        hidden_ref[span, :] = (gate * jax.nn.sigmoid(gate) * up).astype(bf16)
        return carry

    lax.fori_loop(0, rows // step, body, 0)
    for copy in late:
        copy.wait()
    downs = [(weight_refs[r], col, to, w) for r, col, to, w in downs]
    send_terms(at_ref, hidden_ref, downs, outs)


def join_kernel(gate_ref, up_ref, down_ref, a_ref, b_ref, sems):
    width = gate_ref.shape[1]
    cut = a_ref.shape[1] - width
    copies = [
        pltpu.make_async_copy(source, to, sems.at[k])
        for k, (source, to) in enumerate(
            (
                (gate_ref, a_ref.at[:, pl.ds(0, width)]),
                (down_ref.at[:, pl.ds(0, cut)], a_ref.at[:, pl.ds(width, cut)]),
                (up_ref, b_ref.at[:, pl.ds(0, width)]),
                (down_ref.at[:, pl.ds(cut, width - cut)], b_ref.at[:, pl.ds(width, width - cut)]),
            )
        )
    ]
    for copy in copies:
        copy.start()
    for copy in copies:
        copy.wait()


def in_hbm(value):
    return pltpu.with_memory_space_constraint(value, pltpu.HBM)


def join_weights(gate, up, down, cut):
    rows, width = gate.shape
    return pl.pallas_call(
        join_kernel,
        out_shape=[
            jax.ShapeDtypeStruct((rows, width + cut), bf16),
            jax.ShapeDtypeStruct((rows, 2 * width - cut), bf16),
        ],
        in_specs=[pl.BlockSpec(memory_space=pltpu.HBM)] * 3,
        out_specs=[pl.BlockSpec(memory_space=pltpu.VMEM)] * 2,
        scratch_shapes=[pltpu.SemaphoreType.DMA((4,))],
        compiler_params=pltpu.CompilerParams(vmem_limit_bytes=4 * 1024 * 1024),
        name="join",
    )(in_hbm(gate), in_hbm(up), in_hbm(down))


def one_minus_exp(value):
    small = jnp.zeros_like(value)
    for n in (8, 7, 6, 5, 4, 3, 2):
        small = value * (1.0 / n) * (1.0 + small)
    small = value * (1.0 + small)
    return jnp.where(value > -0.5, -small, 1.0 - jnp.exp(value))


def shifted(value, by, fill):
    rows = value.shape[0]
    if by % 8 == 0:
        head = jnp.full((by, value.shape[1]), fill, value.dtype)
        return jnp.concatenate([head, value[: rows - by]], axis=0)
    rolled = pltpu.roll(value, by, 0)
    at = lax.broadcasted_iota(jnp.int32, value.shape, 0)
    return jnp.where(at < by, fill, rolled)


def mixer_kernel(at_ref, *refs, rows, parts):
    blocks = sum(parts)
    x_refs, refs = refs[:blocks], refs[blocks:]
    gain_ref, conv_ref, rate_ref, input_ref, slope_ref, shift_ref, stored_ref = refs[:7]
    outs = refs[7:15]
    normed_ref, mixed_ref, sems, weight_ref = refs[15:19]
    width = weight_ref.shape[1] // 3
    copy = pltpu.make_async_copy(stored_ref, weight_ref, sems.at[0])
    copy.start()
    norm_into(x_refs, parts, at_ref, gain_ref, normed_ref, rows)
    copy.wait()
    both = jnp.dot(normed_ref[...], weight_ref[:, : 2 * width], preferred_element_type=f32)
    lane = both[:, :width].astype(bf16).astype(f32)
    branch = both[:, width:]
    conv = lane * conv_ref[CONV - 1].astype(f32)
    for back in range(1, CONV):
        conv = conv + shifted(lane, back, 0.0) * conv_ref[CONV - 1 - back].astype(f32)
    conv = conv.astype(bf16)
    rate = jax.nn.sigmoid(jnp.dot(conv, rate_ref[...], preferred_element_type=f32))
    admit = jax.nn.sigmoid(jnp.dot(conv, input_ref[...], preferred_element_type=f32))
    at = lax.broadcasted_iota(jnp.int32, (rows, width), 1)
    shift = jnp.where(at < HEAD_DIM, shift_ref[:, 0:1], shift_ref[:, 1:2])
    log_decay = rate_scale * rate * slope_ref[...] + shift
    state = jnp.sqrt(one_minus_exp(2.0 * log_decay)) * admit * conv.astype(f32)
    decay = jnp.exp(log_decay)
    by = 1
    while by < rows:
        state = state + decay * shifted(state, by, 0.0)
        if by * 2 < rows:
            decay = decay * shifted(decay, by, 1.0)
        by *= 2
    gelu = jax.nn.gelu(branch)
    mixed_ref[...] = (state * gelu).astype(bf16)
    send_terms(at_ref, mixed_ref, [(weight_ref, 2 * width, 0, width)], outs)


def call(kernel, at, operands, stored, whole, rows, width, grant=22):
    vmem, hbm = pl.BlockSpec(memory_space=pltpu.VMEM), pl.BlockSpec(memory_space=pltpu.HBM)
    scratch = [
        pltpu.VMEM((rows, D), bf16),
        pltpu.VMEM((rows, width), bf16),
        pltpu.SemaphoreType.DMA((40,)),
        *[pltpu.VMEM(v.shape, v.dtype) for v in whole],
    ]
    outs = pl.pallas_call(
        functools.partial(kernel, rows=rows),
        out_shape=[jax.ShapeDtypeStruct((rows, BLK), bf16)] * 8,
        in_specs=[
            pl.BlockSpec(memory_space=pltpu.SMEM),
            *[hbm if k in stored else vmem for k in range(len(operands))],
        ],
        out_specs=[vmem] * 8,
        scratch_shapes=scratch,
        compiler_params=pltpu.CompilerParams(vmem_limit_bytes=grant * 1024 * 1024),
    )(at, *[in_hbm(v) if k in stored else v for k, v in enumerate(operands)])
    return outs[0::2], outs[1::2]


def block_map(weight):
    zero = jnp.zeros((HEAD_DIM, HEAD_DIM), weight.dtype)
    return jnp.block([[weight[0], zero], [zero, weight[1]]])


def shards(
    tokens,
    first_gain,
    first_gate,
    first_up,
    first_down,
    mix_gain,
    mix_input,
    mix_branch,
    conv_weight,
    rate_weight,
    input_weight,
    decay_param,
    decay_shift,
    mix_output,
    second_gain,
    second_gate,
    second_up,
    second_down,
    final_gain,
):
    rows = tokens.shape[0]
    at = owners()
    width = first_gate.shape[1]
    cut = 384
    first = gather_rows_by_permute(*join_weights(first_gate, first_up, first_down, cut))
    first_columns = ((0, 0), (1, 0), ((0, width, 0, cut), (1, width, cut, width - cut)))
    mix = jnp.concatenate([mix_input, mix_branch, mix_output], axis=1)
    second = jnp.concatenate([second_gate, second_up, second_down], axis=1)
    mix, second, first = lax.optimization_barrier((mix, second, first))
    mix = lax.all_gather(mix, "fs", axis=0, tiled=True)
    second = (lax.all_gather(second, "fs", axis=0, tiled=True),)
    second_columns = ((0, 0), (0, width), ((0, 2 * width, 0, width),))
    gains = [g.reshape(8, 1, BLK) for g in (first_gain, mix_gain, second_gain)]
    slope = jax.nn.log_sigmoid(decay_param).reshape(1, -1)
    rate_map, input_map = block_map(rate_weight), block_map(input_weight)

    def half(stream, gain, weights, columns):
        pieces = len(weights) > 1
        blocks = (gather_row_blocks if pieces else gather_row_halves)(stream)
        parts = WHOLE_PARTS if pieces else HALF_PARTS
        count = len(blocks)
        kept = [0] if pieces else list(range(count - 4, count))
        kernel = functools.partial(
            half_step_kernel, columns=columns, pieces=pieces, parts=parts, stored=kept
        )
        whole = [jax.ShapeDtypeStruct((D, w.shape[1]), bf16) for w in weights[0 :: 8 if pieces else 1]]
        whole += [gain, *[blocks[k] for k in kept]]
        operands = (*blocks, gain, *weights)
        stored = kept + list(range(count, len(operands)))
        terms = call(kernel, at, operands, stored, whole, rows, width)
        return stream.astype(f32) + 0.5 * scatter_row_blocks(*terms)

    stream = half(tokens, gains[0], first, first_columns).astype(bf16)
    blocks = gather_row_halves(stream)
    terms = call(
        functools.partial(mixer_kernel, parts=HALF_PARTS),
        at,
        (*blocks, gains[1], conv_weight, rate_map, input_map, slope, decay_shift, mix),
        [len(blocks) + 6],
        [mix],
        rows,
        mix.shape[1] // 3,
    )
    stream = (stream.astype(f32) + scatter_row_blocks(*terms)).astype(bf16)
    values = half(stream, gains[2], second, second_columns).astype(bf16).astype(f32)
    mine = jnp.sum(values * values, axis=1)
    mine = mine + swap(mine)
    mine = mine + lax.ppermute(mine, "tp_0", [(0, 1), (1, 0), (2, 3), (3, 2)])
    square = mine + lax.ppermute(mine, "tp_0", [(0, 3), (3, 0), (1, 2), (2, 1)])
    scale = lax.rsqrt(square / D + norm_eps)
    return (values * scale[:, None] * final_gain).astype(bf16)


def solution(mesh):
    finer = Mesh(mesh.devices.reshape(mesh.shape["fs"], 4, 2), ("fs", "tp_0", "tp_1"))
    placed = (
        P("fs", TP),
        P(),
        P("fs", TP),
        P("fs", TP),
        P("fs", TP),
        P(),
        P("fs", TP),
        P("fs", TP),
        P(None, TP),
        P(TP, None, None),
        P(TP, None, None),
        P(TP),
        P("fs", TP),
        P("fs", TP),
        P(),
        P("fs", TP),
        P("fs", TP),
        P("fs", TP),
        P(TP),
    )
    return jax.shard_map(shards, mesh=finer, in_specs=placed, out_specs=P("fs", TP), check_vma=False)
```

```python
import functools

import jax
import jax.numpy as jnp
from jax import lax
from jax.experimental import pallas as pl
from jax.experimental.pallas import tpu as pltpu
from jax.sharding import Mesh
from jax.sharding import PartitionSpec as P


D = 2048
BLK = 256
HEAD_DIM = 64
CONV = 4
TP = ("tp_0", "tp_1")
norm_eps = 1e-06
rate_scale = 8.0
bf16 = jnp.bfloat16
f32 = jnp.float32


OFFSETS = ((0, 0), (0, 1), (1, 0), (1, 1), (-1, 0), (-1, 1), (2, 0), (2, 1))


def ring(value, step):
    return lax.ppermute(value, "tp_0", [(i, (i + step) % 4) for i in range(4)])


def swap(value):
    return lax.ppermute(value, "tp_1", [(0, 1), (1, 0)])


def gather_row_blocks(block):
    half = block.shape[0] // 2
    left = ring(block, 1)
    right = ring(block, -1)
    other = swap(block)
    far_top = ring(left[:half], 1)
    far_low = ring(right[half:], -1)
    right_other, left_other = swap(right), swap(left)
    return (
        block,
        other,
        right,
        right_other,
        left,
        left_other,
        far_top,
        far_low,
        swap(far_top),
        swap(far_low),
    )


def gather_row_halves(block):
    half = block.shape[0] // 2
    top, low = block[:half], block[half:]
    left_top = ring(top, 1)
    right_low = ring(low, -1)
    left_low = ring(low, 1)
    right_top = ring(top, -1)
    other = swap(block)
    far_top = ring(left_top, 1)
    far_low = ring(right_low, -1)
    pairs = (right_top, right_low), (left_top, left_low), (far_top, far_low)
    blocks = [block, other]
    for pair in pairs:
        blocks += [*pair, *[swap(h) for h in pair]]
    return tuple(blocks)


WHOLE_PARTS = (1, 1, 1, 1, 1, 1, 2, 2)
HALF_PARTS = (1, 1, 2, 2, 2, 2, 2, 2)


def scatter_row_blocks(mine, others):
    half = mine[0].shape[0] // 2
    got = [swap(o) for o in others]
    own, right, left, far = [mine[k].astype(f32) + got[k].astype(f32) for k in range(4)]
    far = far.astype(bf16)
    got_right = ring(far[:half], 1)
    got_left = ring(far[half:], -1)
    right_low = ring(right[half:].astype(bf16), 1)
    left_top = ring(left[:half].astype(bf16), -1)
    right_top = ring((right[:half] + got_right.astype(f32)).astype(bf16), 1)
    left_low = ring((left[half:] + got_left.astype(f32)).astype(bf16), -1)
    top = own[:half] + right_top.astype(f32) + left_top.astype(f32)
    low = own[half:] + right_low.astype(f32) + left_low.astype(f32)
    return jnp.concatenate([top, low], axis=0)


def fs_ring(value, dz, dx):
    pairs = [
        (z * 4 + x, ((z + dz) % 4) * 4 + (x + dx) % 4) for z in range(4) for x in range(4)
    ]
    return lax.ppermute(value, "fs", pairs)


def gather_rows_by_permute(first, second, first_top, second_top):
    lines = []
    for own, top, near in ((first, first_top, (0, 1)), (second, second_top, (1, 0))):
        got = {step: fs_ring(own, step * near[0], step * near[1]) for step in (1, -1, 2)}
        top = lax.dynamic_update_slice(top, got[1], (own.shape[0], 0))
        low = jnp.concatenate([got[-1], got[2]], axis=0)
        move = lambda v, step: fs_ring(v, step * near[1], step * near[0])
        left_top = move(top, 1)
        right_low = move(low, -1)
        left_low = move(low, 1)
        right_top = move(top, -1)
        far_top = move(left_top, 1)
        far_low = move(right_low, -1)
        lines += [top, low, left_top, left_low, right_top, right_low, far_top, far_low]
    return tuple(lines)


def piece_copies(at_ref, piece_refs, whole_refs, sems):
    z, x = at_ref[8], at_ref[9]
    rows = whole_refs[0].shape[0] // 16
    steps = (0, -1, 1, 2)
    copies = []
    for ref, pieces, outer, inner, along_z in (
        (whole_refs[0], piece_refs[:8], z, x, True),
        (whole_refs[1], piece_refs[8:], x, z, False),
    ):
        for n, piece in enumerate(pieces):
            far = (outer + steps[n // 2] + 4) % 4
            for j in range(2):
                near = (inner + steps[2 * (n % 2) + j] + 4) % 4
                row = far * 4 + near if along_z else near * 4 + far
                to = ref.at[pl.ds(pl.multiple_of(row * rows, rows), rows), :]
                source = piece.at[pl.ds(j * rows, rows), :]
                copies.append(pltpu.make_async_copy(source, to, sems.at[len(copies)]))
    return copies


def owners():
    y, c = lax.axis_index("tp_0"), lax.axis_index("tp_1")
    fs = lax.axis_index("fs")
    blocks = [((y + dy) % 4) * 2 + (c + dc) % 2 for dy, dc in OFFSETS]
    return jnp.stack([*blocks, fs // 4, fs % 4]).astype(jnp.int32)


def norm_into(x_refs, parts, at_ref, gain_ref, normed_ref, rows):
    half = rows // 2
    step = min(256, half)
    starts = [sum(parts[:k]) for k in range(8)]
    for side in range(2):
        refs = [x_refs[at + side * (n - 1)] for at, n in zip(starts, parts)]

        def body(i, carry, side=side, refs=refs):
            near = pl.ds(pl.multiple_of(side * half + i * step, step), step)
            piece = pl.ds(pl.multiple_of(i * step, step), step)
            spans = [near if n == 1 else piece for n in parts]
            square = None
            for r, span in zip(refs, spans):
                v = r[span, :].astype(f32)
                square = v * v if square is None else square + v * v
            scale = lax.rsqrt(jnp.sum(square, axis=1, keepdims=True) / D + norm_eps)
            for k, (r, span) in enumerate(zip(refs, spans)):
                at = at_ref[k]
                lane = pl.ds(pl.multiple_of(at * BLK, BLK), BLK)
                normed_ref[near, lane] = (r[span, :].astype(f32) * scale * gain_ref[at]).astype(bf16)
            return carry

        lax.fori_loop(0, half // step, body, 0)


def dot_t(left, right):
    return lax.dot_general(left, right, (((1,), (1,)), ((), ())), preferred_element_type=f32)


def send_terms(at_ref, value_ref, downs, outs):
    for k in (7, 3, 5, 1, 6, 2, 4, 0):
        at = pl.multiple_of(at_ref[k] * BLK, BLK)
        rows = value_ref.shape[0]
        step = rows if len(downs) > 1 else min(512, rows)
        for lo in range(0, rows, step):
            span = slice(lo, lo + step)
            total = None
            for ref, col, to, width in downs:
                down = ref[pl.ds(at, BLK), col : col + width]
                term = dot_t(value_ref[span, to : to + width], down)
                total = term if total is None else total + term
            outs[k][span, :] = total.astype(bf16)


def half_step_kernel(at_ref, *refs, rows, columns, pieces, parts, stored):
    blocks = sum(parts)
    x_refs, gain_ref, refs = list(refs[:blocks]), refs[blocks], refs[blocks + 1 :]
    count = 16 if pieces else 1
    weight_refs, outs = refs[:count], refs[count : 8 + count]
    normed_ref, hidden_ref, sems, *whole = refs[8 + count :]
    whole, kept_gain, kept = whole[: 1 + pieces], whole[1 + pieces], whole[2 + pieces :]
    width = hidden_ref.shape[1]
    (gate_at, gate_col), (up_at, up_col), downs = columns
    first = [pltpu.make_async_copy(gain_ref, kept_gain, sems.at[32])]
    for n, k in enumerate(stored):
        first.append(pltpu.make_async_copy(x_refs[k], kept[n], sems.at[33 + n]))
        x_refs[k] = kept[n]
    if pieces:
        early, late = piece_copies(at_ref, weight_refs, whole, sems), []
    else:
        spans = [pl.ds(0, 2 * width), pl.ds(2 * width, width)]
        early, late = [
            [pltpu.make_async_copy(weight_refs[0].at[:, p], whole[0].at[:, p], sems.at[k])]
            for k, p in enumerate(spans)
        ]
    for copy in first + early + late:
        copy.start()
    weight_refs = whole
    for copy in first:
        copy.wait()
    norm_into(x_refs, parts, at_ref, kept_gain, normed_ref, rows)
    for copy in early:
        copy.wait()
    step = min(512, rows)

    def body(i, carry):
        span = pl.ds(pl.multiple_of(i * step, step), step)
        normed = normed_ref[span, :]
        gate = jnp.dot(
            normed, weight_refs[gate_at][:, gate_col : gate_col + width], preferred_element_type=f32
        )
        up = jnp.dot(normed, weight_refs[up_at][:, up_col : up_col + width], preferred_element_type=f32)
        hidden_ref[span, :] = (gate * jax.nn.sigmoid(gate) * up).astype(bf16)
        return carry

    lax.fori_loop(0, rows // step, body, 0)
    for copy in late:
        copy.wait()
    downs = [(weight_refs[r], col, to, w) for r, col, to, w in downs]
    send_terms(at_ref, hidden_ref, downs, outs)


def join_kernel(gate_ref, up_ref, down_ref, a_ref, b_ref, a_top_ref, b_top_ref, sems):
    rows, width = gate_ref.shape
    cut = a_ref.shape[1] - width
    left, right = pl.ds(0, width), pl.ds(width, cut)
    rest, own = pl.ds(width, width - cut), pl.ds(0, rows)
    copies = []
    for a, b in ((a_ref, b_ref), (a_top_ref, b_top_ref)):
        for source, to in (
            (gate_ref, a.at[own, left]),
            (down_ref.at[:, pl.ds(0, cut)], a.at[own, right]),
            (up_ref, b.at[own, left]),
            (down_ref.at[:, pl.ds(cut, width - cut)], b.at[own, rest]),
        ):
            copies.append(pltpu.make_async_copy(source, to, sems.at[len(copies)]))
    for copy in copies:
        copy.start()
    for copy in copies:
        copy.wait()


def in_hbm(value):
    return pltpu.with_memory_space_constraint(value, pltpu.HBM)


def join_weights(gate, up, down, cut):
    rows, width = gate.shape
    return pl.pallas_call(
        join_kernel,
        out_shape=[
            jax.ShapeDtypeStruct((times * rows, columns), bf16)
            for times in (1, 2)
            for columns in (width + cut, 2 * width - cut)
        ],
        in_specs=[pl.BlockSpec(memory_space=pltpu.HBM)] * 3,
        out_specs=[pl.BlockSpec(memory_space=pltpu.VMEM)] * 4,
        scratch_shapes=[pltpu.SemaphoreType.DMA((8,))],
        compiler_params=pltpu.CompilerParams(vmem_limit_bytes=4 * 1024 * 1024),
        name="join",
    )(in_hbm(gate), in_hbm(up), in_hbm(down))


def one_minus_exp(value):
    small = jnp.zeros_like(value)
    for n in (8, 7, 6, 5, 4, 3, 2):
        small = value * (1.0 / n) * (1.0 + small)
    small = value * (1.0 + small)
    return jnp.where(value > -0.5, -small, 1.0 - jnp.exp(value))


def shifted(value, by, fill):
    rows = value.shape[0]
    if by % 8 == 0:
        head = jnp.full((by, value.shape[1]), fill, value.dtype)
        return jnp.concatenate([head, value[: rows - by]], axis=0)
    rolled = pltpu.roll(value, by, 0)
    at = lax.broadcasted_iota(jnp.int32, value.shape, 0)
    return jnp.where(at < by, fill, rolled)


def mixer_kernel(at_ref, *refs, rows, parts):
    blocks = sum(parts)
    x_refs, refs = refs[:blocks], refs[blocks:]
    gain_ref, conv_ref, rate_ref, input_ref, slope_ref, shift_ref, stored_ref = refs[:7]
    outs = refs[7:15]
    normed_ref, mixed_ref, sems, weight_ref = refs[15:19]
    width = weight_ref.shape[1] // 3
    copy = pltpu.make_async_copy(stored_ref, weight_ref, sems.at[0])
    copy.start()
    norm_into(x_refs, parts, at_ref, gain_ref, normed_ref, rows)
    copy.wait()
    both = jnp.dot(normed_ref[...], weight_ref[:, : 2 * width], preferred_element_type=f32)
    lane = both[:, :width].astype(bf16).astype(f32)
    branch = both[:, width:]
    conv = lane * conv_ref[CONV - 1].astype(f32)
    for back in range(1, CONV):
        conv = conv + shifted(lane, back, 0.0) * conv_ref[CONV - 1 - back].astype(f32)
    conv = conv.astype(bf16)
    rate = jax.nn.sigmoid(jnp.dot(conv, rate_ref[...], preferred_element_type=f32))
    admit = jax.nn.sigmoid(jnp.dot(conv, input_ref[...], preferred_element_type=f32))
    at = lax.broadcasted_iota(jnp.int32, (rows, width), 1)
    shift = jnp.where(at < HEAD_DIM, shift_ref[:, 0:1], shift_ref[:, 1:2])
    log_decay = rate_scale * rate * slope_ref[...] + shift
    state = jnp.sqrt(one_minus_exp(2.0 * log_decay)) * admit * conv.astype(f32)
    decay = jnp.exp(log_decay)
    by = 1
    while by < rows:
        state = state + decay * shifted(state, by, 0.0)
        if by * 2 < rows:
            decay = decay * shifted(decay, by, 1.0)
        by *= 2
    gelu = jax.nn.gelu(branch)
    mixed_ref[...] = (state * gelu).astype(bf16)
    send_terms(at_ref, mixed_ref, [(weight_ref, 2 * width, 0, width)], outs)


def call(kernel, at, operands, stored, whole, rows, width, grant=22):
    vmem, hbm = pl.BlockSpec(memory_space=pltpu.VMEM), pl.BlockSpec(memory_space=pltpu.HBM)
    scratch = [
        pltpu.VMEM((rows, D), bf16),
        pltpu.VMEM((rows, width), bf16),
        pltpu.SemaphoreType.DMA((40,)),
        *[pltpu.VMEM(v.shape, v.dtype) for v in whole],
    ]
    outs = pl.pallas_call(
        functools.partial(kernel, rows=rows),
        out_shape=[jax.ShapeDtypeStruct((rows, BLK), bf16)] * 8,
        in_specs=[
            pl.BlockSpec(memory_space=pltpu.SMEM),
            *[hbm if k in stored else vmem for k in range(len(operands))],
        ],
        out_specs=[vmem] * 8,
        scratch_shapes=scratch,
        compiler_params=pltpu.CompilerParams(vmem_limit_bytes=grant * 1024 * 1024),
    )(at, *[in_hbm(v) if k in stored else v for k, v in enumerate(operands)])
    return outs[0::2], outs[1::2]


def block_map(weight):
    zero = jnp.zeros((HEAD_DIM, HEAD_DIM), weight.dtype)
    return jnp.block([[weight[0], zero], [zero, weight[1]]])


def shards(
    tokens,
    first_gain,
    first_gate,
    first_up,
    first_down,
    mix_gain,
    mix_input,
    mix_branch,
    conv_weight,
    rate_weight,
    input_weight,
    decay_param,
    decay_shift,
    mix_output,
    second_gain,
    second_gate,
    second_up,
    second_down,
    final_gain,
):
    rows = tokens.shape[0]
    at = owners()
    width = first_gate.shape[1]
    cut = 384
    first = gather_rows_by_permute(*join_weights(first_gate, first_up, first_down, cut))
    first_columns = ((0, 0), (1, 0), ((0, width, 0, cut), (1, width, cut, width - cut)))
    mix = jnp.concatenate([mix_input, mix_branch, mix_output], axis=1)
    second = jnp.concatenate([second_gate, second_up, second_down], axis=1)
    mix, second, first = lax.optimization_barrier((mix, second, first))
    mix = lax.all_gather(mix, "fs", axis=0, tiled=True)
    second = (lax.all_gather(second, "fs", axis=0, tiled=True),)
    second_columns = ((0, 0), (0, width), ((0, 2 * width, 0, width),))
    gains = [g.reshape(8, 1, BLK) for g in (first_gain, mix_gain, second_gain)]
    slope = jax.nn.log_sigmoid(decay_param).reshape(1, -1)
    rate_map, input_map = block_map(rate_weight), block_map(input_weight)

    def half(stream, gain, weights, columns):
        pieces = len(weights) > 1
        blocks = (gather_row_blocks if pieces else gather_row_halves)(stream)
        parts = WHOLE_PARTS if pieces else HALF_PARTS
        count = len(blocks)
        kept = [0] if pieces else list(range(count - 4, count))
        kernel = functools.partial(
            half_step_kernel, columns=columns, pieces=pieces, parts=parts, stored=kept
        )
        whole = [jax.ShapeDtypeStruct((D, w.shape[1]), bf16) for w in weights[0 :: 8 if pieces else 1]]
        whole += [gain, *[blocks[k] for k in kept]]
        operands = (*blocks, gain, *weights)
        stored = kept + list(range(count, len(operands)))
        terms = call(kernel, at, operands, stored, whole, rows, width)
        return stream.astype(f32) + 0.5 * scatter_row_blocks(*terms)

    stream = half(tokens, gains[0], first, first_columns).astype(bf16)
    blocks = gather_row_halves(stream)
    terms = call(
        functools.partial(mixer_kernel, parts=HALF_PARTS),
        at,
        (*blocks, gains[1], conv_weight, rate_map, input_map, slope, decay_shift, mix),
        [len(blocks) + 6],
        [mix],
        rows,
        mix.shape[1] // 3,
    )
    stream = (stream.astype(f32) + scatter_row_blocks(*terms)).astype(bf16)
    values = half(stream, gains[2], second, second_columns).astype(bf16).astype(f32)
    mine = jnp.sum(values * values, axis=1)
    mine = mine + swap(mine)
    mine = mine + lax.ppermute(mine, "tp_0", [(0, 1), (1, 0), (2, 3), (3, 2)])
    square = mine + lax.ppermute(mine, "tp_0", [(0, 3), (3, 0), (1, 2), (2, 1)])
    scale = lax.rsqrt(square / D + norm_eps)
    return (values * scale[:, None] * final_gain).astype(bf16)


def solution(mesh):
    finer = Mesh(mesh.devices.reshape(mesh.shape["fs"], 4, 2), ("fs", "tp_0", "tp_1"))
    placed = (
        P("fs", TP),
        P(),
        P("fs", TP),
        P("fs", TP),
        P("fs", TP),
        P(),
        P("fs", TP),
        P("fs", TP),
        P(None, TP),
        P(TP, None, None),
        P(TP, None, None),
        P(TP),
        P("fs", TP),
        P("fs", TP),
        P(),
        P("fs", TP),
        P("fs", TP),
        P("fs", TP),
        P(TP),
    )
    return jax.shard_map(
        shards, mesh=finer, in_specs=placed, out_specs=P("fs", TP), check_vma=False
    )
```
